32 devices in a mesh: sp: 8 (over z, y), dp: 4 (over x, core).
Axes of the slice: x: 2, y: 2, z: 4, core: 2. Of those that a mesh axis runs over, the one named last changes fastest.
Arguments:
- residual: bfloat16 [4, 1024, 2048], P('dp', 'sp'), may hold values from -6 to 6
- query_maps: bfloat16 [4, 1024, 2048], P('dp', 'sp'), may hold values from -200 to 200
- key_maps: bfloat16 [4, 1024, 2048], P('dp', 'sp'), may hold values from -200 to 200
- value_rows: bfloat16 [4, 1024, 2048], P('dp', 'sp'), may hold values from -6 to 6
- lambdas: float32 [16], replicated, may hold values from 0.3 to 0.8
- head_gain: float32 [2048], replicated, may hold values from 0.1 to 1.9
- out_weight: bfloat16 [2048, 2048], replicated, may hold values from -0.125 to 0.125
- ffn_gain: float32 [2048], replicated, may hold values from 0.1 to 1.9
- routes: int32 [4, 1024, 2], P('dp', 'sp'), may hold values from 0 to 31, all different within a row; in each aligned block of 128 rows (0 to 127, 128 to 255, ..., all dimensions but the last counted through in order) at most 16 rows name the same one
- route_weights: float32 [4, 1024, 2], P('dp', 'sp'), may hold values from 0.2 to 1
- expert_gate: bfloat16 [32, 2048, 1024], P(('sp', 'dp')), may hold values from -0.125 to 0.125
- expert_up: bfloat16 [32, 2048, 1024], P(('sp', 'dp')), may hold values from -0.125 to 0.125
- expert_down: bfloat16 [32, 1024, 2048], P(('sp', 'dp')), may hold values from -0.1875 to 0.1875
Outputs:
- layer_out: bfloat16 [4, 1024, 2048], P('dp', 'sp')
The draws below stay inside these ranges and needn't reach their ends.
Inputs may be any that keep to these rules, and one draw needn't show every extreme that they name: `routes`: A token's 2 experts differ; among the 128 rows of one device no expert is named more than 16 times, and in every draw some expert is named exactly 16 times by one device's rows.
All inputs are finite; a program needn't handle non-finite values.
Results may differ from the reference program's by a relative error of at most 0.012.
Values may be sent and summed in bfloat16 or wider, within the bound.
A program may use at most 128 MiB of HBM per device.

```python
import math
import jax
import jax.numpy as jnp
import numpy as np
from jax import lax

D = 2048
HEADS = 16
HD = 64
VD = 128
FF = 1024
TOPK = 2
TOK_DEV = 128
SEQ = 1024
EXPERTS = 32
CAP = 16
N_DP = 4


def base_keys(key):
    return 1.3 * jax.random.normal(jax.random.fold_in(key, 11), (N_DP, SEQ, HEADS * 2 * HD), jnp.float32)


def draw_key_maps(key, part):
    drawn = base_keys(key)
    return drawn.astype(jnp.bfloat16)


def draw_query_maps(key, part):
    drawn = 1.3 * jax.random.normal(jax.random.fold_in(key, 21), (N_DP, SEQ, HEADS * 2 * HD), jnp.float32)
    return drawn.astype(jnp.bfloat16)


def shard_levels(key, extent, split, least, largest):
    gain = 1.0
    for axis_at, shards_of in split:
        steps = jax.random.uniform(jax.random.fold_in(jax.random.fold_in(key, 6), axis_at), (shards_of,), jnp.float32, least / len(split), largest / len(split))
        gain = gain * jnp.repeat(jnp.exp(steps), extent[axis_at] // shards_of).reshape((-1,) + (1,) * (len(extent) - 1 - axis_at))
    return gain


def shared_out(own_key, own, number, rows, number_of, top, limit, skew):
    sequence = jax.random.permutation(own_key, number_of)
    crowded, usual = load_shares(number_of, rows * top, limit, skew, True), load_shares(number_of, rows * top, limit, skew, False)
    places = jnp.arange(number_of)

    def named(lengths, turn):
        used = int((lengths > 0).sum())
        fixed = max(1, used // 4)
        passed = fixed + (places - fixed + turn * (used - fixed)) % max(1, number_of - fixed)
        return jnp.zeros((number_of,), jnp.int32).at[sequence[jnp.where(places < fixed, places, passed)]].set(jnp.asarray(lengths, jnp.int32))

    lengths = jnp.where(number % 4 == 0, named(crowded, number // 4), named(usual, number - number // 4 - 1))
    mixed = jax.random.permutation(jax.random.fold_in(own, 3), number_of)
    giver, taker = mixed[0:number_of // 2 * 2:2], mixed[1:number_of // 2 * 2:2]
    slack = jnp.minimum(lengths[giver] - 1, limit - lengths[taker]) // 2
    slack = jnp.where((giver == sequence[0]) | (taker == sequence[0]) | (lengths[taker] == 0), 0, jnp.maximum(slack, 0))
    passed = jax.random.randint(jax.random.fold_in(own, 4), (number_of // 2,), 0, 1 << 20) % (slack + 1)
    lengths = lengths.at[giver].add(-passed).at[taker].add(passed)
    members = jnp.searchsorted(jnp.cumsum(lengths), jnp.arange(rows * top), side="right").astype(jnp.int32)
    table = members.reshape(top, rows).T
    table = table[jax.random.permutation(jax.random.fold_in(own, 1), rows)]
    turn = jax.random.randint(jax.random.fold_in(own, 2), (rows, 1), 0, top)
    return jnp.take_along_axis(table, (jnp.arange(top)[None, :] + turn) % top, axis=1)


def load_shares(count, total, bound, slope, full):
    weights = [(1 << 20) // math.isqrt(rank ** slope) + 1 for rank in range(1, count + 1)]
    largest = bound if full else min(bound, max(-(-total // count), total * weights[0] // sum(weights)))
    least = 1 if total - largest >= count - 1 else 0
    holding, spare = [largest] + [least] * (count - 1), total - largest - least * (count - 1)
    while spare > 0:
        candidates = [i for i in range(1, count) if holding[i] < largest] or [i for i in range(1, count) if holding[i] < bound]
        whole, remaining = sum([weights[i] for i in candidates]), spare
        for i in candidates:
            extra = min(bound - holding[i], max(1, remaining * weights[i] // whole), spare)
            holding[i] = holding[i] + extra
            spare = spare - extra
    return np.array(holding)


def scatter_about(rng, extent, scale, bound, shards=(), kind=jnp.bfloat16):
    gain = shard_levels(rng, extent, shards, -0.22, 0.18) if shards else 1.0
    values = jax.random.normal(rng, extent, jnp.float32) * scale * gain
    return jnp.minimum(jnp.maximum(values, -bound), bound).astype(kind)


def setup_inputs(seed: int = 0) -> dict:
    arg_keys = jax.random.split(jax.random.key(seed), 14)
    residual = scatter_about(arg_keys[0], (N_DP, SEQ, D), 1.0, 6.0, ((0, 4), (1, 8)))
    query_maps = draw_query_maps(jax.random.fold_in(arg_keys[13], 71), 0)
    key_maps = draw_key_maps(jax.random.fold_in(arg_keys[13], 71), 0)
    value_rows = scatter_about(arg_keys[3], (N_DP, SEQ, HEADS * VD), 1.0, 6.0, ((0, 4), (1, 8)))
    lambdas = jnp.clip(jax.random.uniform(arg_keys[4], (HEADS,), jnp.float32, 0.3, 0.8), 0.3, 0.8)
    head_gain = jnp.clip(1.0 + 0.18 * jax.random.normal(arg_keys[5], (HEADS * VD,), jnp.float32), 0.1, 1.9)
    out_weight = scatter_about(arg_keys[6], (HEADS * VD, D), (HEADS * VD) ** -0.5, 0.125)
    ffn_gain = jnp.clip(1.0 + 0.18 * jax.random.normal(arg_keys[7], (D,), jnp.float32), 0.1, 1.9)
    routes_keys = jax.random.split(jax.random.fold_in(arg_keys[8], 1), N_DP * SEQ // TOK_DEV)
    routes_turns = jax.random.permutation(jax.random.fold_in(arg_keys[8], 3), N_DP * SEQ // TOK_DEV)
    routes = jax.vmap(lambda own, number: shared_out(jax.random.fold_in(arg_keys[8], 2), own, number, TOK_DEV, EXPERTS, TOPK, CAP, 2))(routes_keys, routes_turns).reshape((N_DP, SEQ, TOPK))
    route_weights = jnp.clip(jnp.exp(math.log(1.0) - 1.609438 * jax.random.uniform(arg_keys[9], (N_DP, SEQ, TOPK), jnp.float32) ** shard_levels(arg_keys[9], (N_DP, SEQ, TOPK), ((0, 4), (1, 8)), -0.2, 0.2)), 0.2, 1.0)
    expert_gate = scatter_about(arg_keys[10], (EXPERTS, D, FF), D ** -0.5, 0.125, ((0, 32),))
    expert_up = scatter_about(arg_keys[11], (EXPERTS, D, FF), D ** -0.5, 0.125, ((0, 32),))
    expert_down = scatter_about(arg_keys[12], (EXPERTS, FF, D), FF ** -0.5, 0.1875, ((0, 32),))
    return {"residual": residual, "query_maps": query_maps, "key_maps": key_maps, "value_rows": value_rows, "lambdas": lambdas, "head_gain": head_gain, "out_weight": out_weight, "ffn_gain": ffn_gain, "routes": routes, "route_weights": route_weights, "expert_gate": expert_gate, "expert_up": expert_up, "expert_down": expert_down}


eps = 1e-06

def attend_head(query_head, key_head, value_head, lam_head, gain_head):
    length = query_head.shape[0]
    block_rows = min(512, length)
    count_blocks = length // block_rows
    scaling = query_head.shape[-1] ** (-0.5)
    query_blocks = query_head.reshape(count_blocks, block_rows, 2, query_head.shape[-1])
    keys_wide = key_head.astype(jnp.float32)

    def one_block(query_block):
        scores = jnp.einsum('qmd,kmd->mqk', query_block.astype(jnp.float32), keys_wide) * scaling
        probabilities = jax.nn.softmax(scores, axis=-1)
        mixed_map = (probabilities[0] - lam_head * probabilities[1]).astype(jnp.bfloat16)
        head_out = jnp.dot(mixed_map, value_head, preferred_element_type=jnp.float32)
        normed = head_out * lax.rsqrt(lax.optimization_barrier(jnp.mean(head_out * head_out, axis=-1, keepdims=True)) + eps)
        return (normed * gain_head * 0.8).astype(jnp.bfloat16)
    return lax.map(one_block, query_blocks).reshape(length, value_head.shape[-1])

def reference(residual, query_maps, key_maps, value_rows, lambdas, head_gain, out_weight, ffn_gain, routes, route_weights, expert_gate, expert_up, expert_down):
    items = N_DP * HEADS
    query_items = query_maps.reshape(N_DP, SEQ, HEADS, 2, HD).transpose(0, 2, 1, 3, 4).reshape(items, SEQ, 2, HD)
    key_items = key_maps.reshape(N_DP, SEQ, HEADS, 2, HD).transpose(0, 2, 1, 3, 4).reshape(items, SEQ, 2, HD)
    value_items = value_rows.reshape(N_DP, SEQ, HEADS, VD).transpose(0, 2, 1, 3).reshape(items, SEQ, VD)
    lam_items = jnp.tile(lambdas, N_DP)
    gain_items = jnp.tile(head_gain.reshape(HEADS, VD), (N_DP, 1))

    def per_item(packed):
        return attend_head(packed[0], packed[1], packed[2], packed[3], packed[4])
    attended = lax.map(per_item, (query_items, key_items, value_items, lam_items, gain_items))
    attended = attended.reshape(N_DP, HEADS, SEQ, VD).transpose(0, 2, 1, 3).reshape(N_DP * SEQ, HEADS * VD)
    total_rows = N_DP * SEQ
    projected = jnp.dot(attended, out_weight, preferred_element_type=jnp.float32)
    residual_mid = (residual.reshape(total_rows, D).astype(jnp.float32) + projected).astype(jnp.bfloat16)
    middle = residual_mid.astype(jnp.float32)
    expert_input = (middle * lax.rsqrt(lax.optimization_barrier(jnp.mean(middle * middle, axis=-1, keepdims=True)) + eps) * ffn_gain).astype(jnp.bfloat16)
    count_blocks = total_rows // TOK_DEV
    block_routes = routes.reshape(count_blocks, TOK_DEV * TOPK)

    def rank_block(route_block):
        onehot = (route_block[:, None] == jnp.arange(EXPERTS, dtype=jnp.int32)[None, :]).astype(jnp.int32)
        before = jnp.cumsum(onehot, axis=0) - onehot
        return lax.optimization_barrier(jnp.sum(before * onehot, axis=1))
    rank_of = lax.map(rank_block, block_routes).reshape(-1)
    flat_routes = routes.reshape(-1).astype(jnp.int32)
    token_of = (jnp.arange(total_rows * TOPK, dtype=jnp.int32) // TOPK).astype(jnp.int32)
    column = token_of // TOK_DEV * CAP + rank_of
    slot_table = jnp.full((EXPERTS, count_blocks * CAP), total_rows, jnp.int32).at[flat_routes, column].set(token_of)
    weight_table = jnp.zeros((EXPERTS, count_blocks * CAP), jnp.float32).at[flat_routes, column].set(route_weights.reshape(-1))
    padded_input = jnp.concatenate([expert_input, jnp.zeros((1, D), jnp.bfloat16)], axis=0)

    def per_expert(accumulated, packed):
        table_row, weight_row, gate_weight, up_weight, down_weight = packed
        row_block = padded_input[table_row]
        gate_part = jnp.dot(row_block, gate_weight, preferred_element_type=jnp.float32)
        up_part = jnp.dot(row_block, up_weight, preferred_element_type=jnp.float32)
        hidden = (jax.nn.silu(gate_part) * up_part).astype(jnp.bfloat16)
        expert_out = jnp.dot(hidden, down_weight, preferred_element_type=jnp.float32).astype(jnp.bfloat16)
        accumulated = accumulated.at[table_row].add(weight_row[:, None] * expert_out.astype(jnp.float32))
        return (accumulated, None)
    start_sum = jnp.zeros((total_rows + 1, D), jnp.float32)
    accumulated, _ = lax.scan(per_expert, start_sum, (slot_table, weight_table, expert_gate, expert_up, expert_down))
    layer_out = (middle + accumulated[:total_rows]).astype(jnp.bfloat16)
    return layer_out.reshape(N_DP, SEQ, D)
```

```python
import functools
import math

import jax
import jax.numpy as jnp
from jax import lax
from jax.experimental import pallas as pl
from jax.experimental.pallas import tpu as pltpu
from jax.sharding import PartitionSpec as P

D = 2048
HEADS = 16
HD = 64
VD = 128


eps = 1e-06


def attend_head(query_head, key_head, value_head, lam_head, gain_head):
    length = query_head.shape[0]
    block_rows = min(512, length)
    count_blocks = length // block_rows
    scaling = query_head.shape[-1] ** (-0.5)
    query_blocks = query_head.reshape(count_blocks, block_rows, 2, query_head.shape[-1])

    def one_block(query_block):
        scores = (
            jnp.einsum("qmd,kmd->mqk", query_block, key_head, preferred_element_type=jnp.float32)
            * scaling
        )
        probabilities = jax.nn.softmax(scores, axis=-1)
        mixed_map = (probabilities[0] - lam_head * probabilities[1]).astype(jnp.bfloat16)
        head_out = jnp.dot(mixed_map, value_head, preferred_element_type=jnp.float32)
        normed = head_out * lax.rsqrt(jnp.mean(head_out * head_out, axis=-1, keepdims=True) + eps)
        return (normed * gain_head * 0.8).astype(jnp.bfloat16)

    return lax.map(one_block, query_blocks).reshape(length, value_head.shape[-1])


def on_device(
    residual,
    query_maps,
    key_maps,
    value_rows,
    lambdas,
    head_gain,
    out_weight,
    ffn_gain,
    routes,
    route_weights,
    expert_gate,
    expert_up,
    expert_down,
):
    count_sp = lax.axis_size("sp")
    count_dp = lax.axis_size("dp")
    heads_here = HEADS // count_sp
    queries, keys_all, values_all = (
        lax.all_to_all(query_maps, "sp", split_axis=2, concat_axis=1, tiled=True),
        lax.all_to_all(key_maps, "sp", split_axis=2, concat_axis=1, tiled=True),
        lax.all_to_all(value_rows, "sp", split_axis=2, concat_axis=1, tiled=True),
    )
    first_head = lax.axis_index("sp") * heads_here
    lam_here = lax.dynamic_slice_in_dim(lambdas, first_head, heads_here)
    gain_here = lax.dynamic_slice_in_dim(head_gain, first_head * VD, heads_here * VD)
    outputs = []
    for head_index in range(heads_here):
        query_head = queries[0, :, head_index * 2 * HD : (head_index + 1) * 2 * HD].reshape(
            -1, 2, HD
        )
        key_head = keys_all[0, :, head_index * 2 * HD : (head_index + 1) * 2 * HD].reshape(
            -1, 2, HD
        )
        value_head = values_all[0, :, head_index * VD : (head_index + 1) * VD]
        gain_head = gain_here[head_index * VD : (head_index + 1) * VD]
        outputs.append(
            attend_head(query_head, key_head, value_head, lam_here[head_index], gain_head)
        )
    attended = jnp.concatenate(outputs, axis=1)[None]
    returned_heads = lax.all_to_all(attended, "sp", split_axis=1, concat_axis=2, tiled=True)
    projected = jnp.dot(returned_heads[0], out_weight, preferred_element_type=jnp.float32)
    residual_mid = (residual[0].astype(jnp.float32) + projected).astype(jnp.bfloat16)
    middle = residual_mid.astype(jnp.float32)
    expert_input = (
        middle * lax.rsqrt(jnp.mean(middle * middle, axis=-1, keepdims=True) + eps) * ffn_gain
    ).astype(jnp.bfloat16)
    tok_rows = residual.shape[1]
    experts_all = count_sp * count_dp
    capacity = max(2, 4 * tok_rows // experts_all)
    flat_routes = routes[0].reshape(-1)
    flat_weights = route_weights[0].reshape(-1)
    onehot = (flat_routes[:, None] == jnp.arange(experts_all, dtype=jnp.int32)[None, :]).astype(
        jnp.int32
    )
    before = jnp.cumsum(onehot, axis=0) - onehot
    rank_of = jnp.sum(before * onehot, axis=1)
    slot = flat_routes * capacity + rank_of
    token_of = jnp.arange(flat_routes.shape[0], dtype=jnp.int32) // routes.shape[2]
    slot_token = jnp.full((experts_all * capacity,), tok_rows, jnp.int32).at[slot].set(token_of)
    padded_input = jnp.concatenate([expert_input, jnp.zeros((1, D), jnp.bfloat16)], axis=0)
    buffer = padded_input[slot_token].reshape(experts_all, capacity, D)
    received = lax.all_to_all(buffer, ("sp", "dp"), split_axis=0, concat_axis=0, tiled=True)
    row_block = received.reshape(-1, D)
    gate_part = jnp.dot(row_block, expert_gate[0], preferred_element_type=jnp.float32)
    up_part = jnp.dot(row_block, expert_up[0], preferred_element_type=jnp.float32)
    hidden = (jax.nn.silu(gate_part) * up_part).astype(jnp.bfloat16)
    expert_out = jnp.dot(hidden, expert_down[0], preferred_element_type=jnp.float32).astype(
        jnp.bfloat16
    )
    returned = lax.all_to_all(
        expert_out.reshape(received.shape), ("sp", "dp"), split_axis=0, concat_axis=0, tiled=True
    )
    picked = returned.reshape(experts_all * capacity, D)[slot]
    weighted = (picked.astype(jnp.float32) * flat_weights[:, None]).reshape(
        tok_rows, routes.shape[2], D
    )
    layer_out = (middle + jnp.sum(weighted, axis=1)).astype(jnp.bfloat16)
    return layer_out[None]


MESH = pl.DeviceIdType.MESH
VMEM_LIMIT = 60 * 1024 * 1024


def slot_masks(routes, first_expert, experts_all, experts_here, capacity):
    rows = routes.shape[1]
    first, second = routes[0:1, :], routes[1:2, :]
    experts = lax.broadcasted_iota(jnp.int32, (experts_all, rows), 0)
    named_first, named_second = experts == first, experts == second
    named = jnp.where(named_first | named_second, 1.0, 0.0).astype(jnp.bfloat16)
    earlier = lax.broadcasted_iota(jnp.int32, (rows, rows), 0) < lax.broadcasted_iota(
        jnp.int32, (rows, rows), 1
    )
    before = jnp.dot(
        named, jnp.where(earlier, 1.0, 0.0).astype(jnp.bfloat16), preferred_element_type=jnp.float32
    )
    slots = lax.broadcasted_iota(jnp.int32, (experts_here * capacity, rows), 0)
    masks = []
    for route, chosen in ((first, named_first), (second, named_second)):
        rank = jnp.sum(jnp.where(chosen, before, 0.0), axis=0, keepdims=True).astype(jnp.int32)
        masks.append(slots == (route - first_expert) * capacity + rank)
    return masks


def mixer_kernel(
    count_sp,
    lam_ref,
    q_ref,
    k_ref,
    v_ref,
    residual_ref,
    gain_ref,
    ow_hbm,
    fgain_ref,
    mid_ref,
    xin_ref,
    qh,
    kh,
    vh,
    outs,
    att,
    ow,
    send_sem,
    recv_sem,
    back_send,
    back_recv,
    local_sem,
    ow_sem,
):
    me = lax.axis_index("sp")
    rows = q_ref.shape[0]
    heads_here = HEADS // count_sp
    length = rows * count_sp
    sources = ((k_ref, kh), (q_ref, qh), (v_ref, vh))

    barrier = pltpu.get_barrier_semaphore()

    def greet(d, carry):
        pl.semaphore_signal(
            barrier, inc=1, device_id={"sp": lax.rem(me + d, count_sp)}, device_id_type=MESH
        )
        return carry

    lax.fori_loop(1, count_sp, greet, 0)
    weight_copy = pltpu.make_async_copy(ow_hbm, ow, ow_sem)
    my_rows = pl.ds(pl.multiple_of(me * rows, rows), rows)

    def local_copy(t, h):
        src, dst = sources[t]
        cols = pl.ds(pl.multiple_of((me * heads_here + h) * VD, VD), VD)
        return pltpu.make_async_copy(src.at[:, cols], dst.at[h, my_rows, :], local_sem.at[t, h])

    def outgoing(t, h, d):
        src, dst = sources[t]
        peer = lax.rem(me + d, count_sp)
        cols = pl.ds(pl.multiple_of((peer * heads_here + h) * VD, VD), VD)
        return pltpu.make_async_remote_copy(
            src_ref=src.at[:, cols],
            dst_ref=dst.at[h, my_rows, :],
            send_sem=send_sem.at[t, h, d],
            recv_sem=recv_sem.at[t, h, d],
            device_id={"sp": peer},
            device_id_type=MESH,
        )

    pl.semaphore_wait(barrier, count_sp - 1)
    for h in range(heads_here):

        for t in (0, 2, 1):

            def start_all(i, carry, t=t, h=h):
                outgoing(t, h, 1 + lax.rem(i + count_sp // 2 - 1, count_sp - 1)).start()
                return carry

            lax.fori_loop(0, count_sp - 1, start_all, 0)
            local_copy(t, h).start()
    weight_copy.start()

    def returning(h, p, d):
        dst_cols = pl.ds(pl.multiple_of((me * heads_here + h) * VD, VD), VD)
        return pltpu.make_async_remote_copy(
            src_ref=outs.at[h, pl.ds(pl.multiple_of(p * rows, rows), rows), :],
            dst_ref=att.at[:, dst_cols],
            send_sem=back_send.at[h, d],
            recv_sem=back_recv.at[h, d],
            device_id={"sp": p},
            device_id_type=MESH,
        )

    factor = HD ** (-0.5) * math.log2(math.e)
    lanes = lax.broadcasted_iota(jnp.int32, (rows, VD), 1)
    for h in range(heads_here):
        for t in range(3):
            local_copy(t, h).wait()
        for t in (0, 2):

            def arrived(d, carry, t=t, h=h):
                outgoing(t, h, d).wait_recv()
                return carry

            lax.fori_loop(1, count_sp, arrived, 0)
        head = me * heads_here + h
        lam = lam_ref[head]
        gain = gain_ref[pl.ds(head, 1), :]

        def attend(p, h=h, lam=lam, gain=gain):
            at = pl.ds(pl.multiple_of(p * rows, rows), rows)
            q = qh[h, at, :]
            zero = jnp.zeros_like(q)
            both = jnp.concatenate(
                [jnp.where(lanes < HD, q, zero), jnp.where(lanes < HD, zero, q)], axis=0
            )
            scores = lax.dot_general(
                both, kh[h], (((1,), (1,)), ((), ())), preferred_element_type=jnp.float32
            )
            top = jnp.max(scores, axis=1, keepdims=True)
            e = jnp.exp2((scores - top) * factor)
            total = jnp.sum(e, axis=1, keepdims=True)
            total_1, total_2 = total[:rows], total[rows:]
            share = lam * total_1 / total_2
            mixed = (e[:rows] - share * e[rows:]).astype(jnp.bfloat16)
            head_out = jnp.dot(mixed, vh[h], preferred_element_type=jnp.float32) / total_1
            normed = head_out * lax.rsqrt(
                jnp.mean(head_out * head_out, axis=-1, keepdims=True) + eps
            )
            return (normed * gain * 0.8).astype(jnp.bfloat16)

        def step(i, carry, h=h, attend=attend):
            d = 1 + lax.rem(i + count_sp // 2 - 1, count_sp - 1)
            p = lax.rem(me + count_sp - d, count_sp)
            outgoing(1, h, d).wait_recv()
            outs[h, pl.ds(pl.multiple_of(p * rows, rows), rows), :] = attend(p)
            returning(h, p, d).start()
            return carry

        lax.fori_loop(0, count_sp - 1, step, 0)
        att[:, pl.ds(pl.multiple_of(head * VD, VD), VD)] = attend(me)

    weight_copy.wait()
    for h in range(heads_here):

        def back(d, carry, h=h):
            returning(h, lax.rem(me + count_sp - d, count_sp), d).wait_recv()
            return carry

        lax.fori_loop(1, count_sp, back, 0)

    tile = 512
    square = jnp.zeros((rows, 1), jnp.float32)
    for j in range(D // tile):
        cols = slice(j * tile, (j + 1) * tile)
        projected = jnp.dot(att[...], ow[:, cols], preferred_element_type=jnp.float32)
        middle = (residual_ref[:, cols].astype(jnp.float32) + projected).astype(jnp.bfloat16)
        mid_ref[:, cols] = middle
        wide = middle.astype(jnp.float32)
        square = square + jnp.sum(wide * wide, axis=1, keepdims=True)
    scale = lax.rsqrt(square / D + eps)
    xin_ref[...] = (mid_ref[...].astype(jnp.float32) * scale * fgain_ref[...]).astype(jnp.bfloat16)

    for h in range(heads_here):

        def drain(d, carry, h=h):
            for t in range(3):
                outgoing(t, h, d).wait_send()
            returning(h, lax.rem(me + count_sp - d, count_sp), d).wait_send()
            return carry

        lax.fori_loop(1, count_sp, drain, 0)


PARTS = 4
LINE = 4


def experts_kernel(
    count_sp,
    count_dp,
    capacity,
    xin_ref,
    mid_ref,
    routes_ref,
    weights_ref,
    gate_hbm,
    up_hbm,
    down_hbm,
    out_ref,
    routes_far,
    weights_far,
    xin_far,
    partial,
    inbox,
    near_sum,
    buffer,
    received,
    results,
    returned,
    gate,
    up,
    down,
    hidden,
    table_send,
    table_recv,
    line_send,
    line_recv,
    sum_send,
    sum_recv,
    send_sem,
    recv_sem,
    back_send,
    back_recv,
    own_sem,
    weight_sem,
):
    count = count_sp * count_dp
    inner = count_sp // LINE
    peers = inner * count_dp
    sp = lax.axis_index("sp")
    z, y = sp // inner, lax.rem(sp, inner)
    me = y * count_dp + lax.axis_index("dp")
    width = gate.shape[1]
    span = D // PARTS
    side = z // 2
    inside = (z * (LINE - 1 - z)) // 2
    mate_z = z + 1 - 2 * lax.rem(z, 2)
    near_z = 2 - side
    last_z = 3 - 3 * side

    def on_line(other):
        return {"sp": other * inner + y}

    def on_plane(p):
        return {"sp": z * inner + p // count_dp, "dp": lax.rem(p, count_dp)}

    barrier = pltpu.get_barrier_semaphore()

    def greet(d, carry):
        pl.semaphore_signal(
            barrier, inc=1, device_id=on_plane(lax.rem(me + d, peers)), device_id_type=MESH
        )
        return carry

    lax.fori_loop(1, peers, greet, 0)
    for other in (mate_z, near_z, last_z):
        pl.semaphore_signal(barrier, inc=1, device_id=on_line(other), device_id_type=MESH)

    def rows_of(i):
        return pl.ds(pl.multiple_of(i * capacity, capacity), capacity)

    def part(c):
        return pl.ds(c * span, span)

    def offset(i):
        return 1 + lax.rem(i + peers // 2 - 2, peers - 1)

    def to_line(src, dst, sent, got, other):
        return pltpu.make_async_remote_copy(
            src_ref=src,
            dst_ref=dst,
            send_sem=sent,
            recv_sem=got,
            device_id=on_line(other),
            device_id_type=MESH,
        )

    tables = []
    for k, (other, slot) in enumerate(((mate_z, 0), (near_z, 2 - inside), (last_z, 2 - inside))):
        for t, (src, dst) in enumerate(((routes_ref, routes_far), (weights_ref, weights_far))):
            tables.append(
                to_line(src, dst.at[slot], table_send.at[k, t], table_recv.at[slot, t], other)
            )

    def tables_here(s):
        for t, (src, dst) in enumerate(((routes_ref, routes_far), (weights_ref, weights_far))):
            to_line(
                src, dst.at[s - 1], table_send.at[0, t], table_recv.at[s - 1, t], mate_z
            ).wait_recv()

    def to_mate(c):
        return to_line(
            xin_ref.at[:, part(c)],
            xin_far.at[0, :, part(c)],
            line_send.at[0, c],
            line_recv.at[0, c],
            mate_z,
        )

    def to_near(c):
        slot = 2 - inside
        return to_line(
            xin_ref.at[:, part(c)],
            xin_far.at[slot, :, part(c)],
            line_send.at[1, c],
            line_recv.at[slot, c],
            near_z,
        )

    def relay(s, c):
        held = xin_far.at[s - 1, :, part(c)]
        return to_line(held, held, line_send.at[s, c], line_recv.at[s - 1, c], mate_z)

    def line_here(s, c):
        held = xin_far.at[s - 1, :, part(c)]
        to_line(held, held, line_send.at[0, c], line_recv.at[s - 1, c], mate_z).wait_recv()

    def sum_out(s, c):
        if s == 1:
            other, slot = mate_z, 0
        else:
            beyond = near_z if s == 2 else last_z
            other = inside * beyond + (1 - inside) * mate_z
            slot = inside + (1 - inside) * s
        return to_line(
            partial.at[s - 1, :, part(c)],
            inbox.at[slot, :, part(c)],
            sum_send.at[s - 1, c],
            sum_recv.at[slot, c],
            other,
        )

    def sum_here(slot, c):
        held = inbox.at[slot, :, part(c)]
        to_line(held, held, sum_send.at[0, c], sum_recv.at[slot, c], mate_z).wait_recv()

    def outgoing(s, c, i):
        p = lax.rem(me + offset(i), peers)
        return pltpu.make_async_remote_copy(
            src_ref=buffer.at[s, rows_of(p), part(c)],
            dst_ref=received.at[s, rows_of(i), part(c)],
            send_sem=send_sem.at[s, c, i],
            recv_sem=recv_sem.at[s, c, i],
            device_id=on_plane(p),
            device_id_type=MESH,
        )

    def returning(s, c, i):
        p = lax.rem(me + peers - offset(i), peers)
        return pltpu.make_async_remote_copy(
            src_ref=results.at[s, rows_of(i), part(c)],
            dst_ref=returned.at[s, rows_of(me), part(c)],
            send_sem=back_send.at[s, c, i],
            recv_sem=back_recv.at[s, c, i],
            device_id=on_plane(p),
            device_id_type=MESH,
        )

    def own_in(s, c):
        return pltpu.make_async_copy(
            buffer.at[s, rows_of(me), part(c)],
            received.at[s, rows_of(0), part(c)],
            own_sem.at[0, s, c],
        )

    def own_out(s, c):
        return pltpu.make_async_copy(
            results.at[s, rows_of(0), part(c)],
            returned.at[s, rows_of(me), part(c)],
            own_sem.at[1, s, c],
        )

    loads = [
        pltpu.make_async_copy(src, dst, weight_sem.at[j])
        for j, (src, dst) in enumerate(((gate_hbm, gate), (up_hbm, up), (down_hbm, down)))
    ]
    for load in loads:
        load.start()

    def each(do):
        def body(i, carry):
            do(i)
            return carry

        lax.fori_loop(1, peers, body, 0)

    pl.semaphore_wait(barrier, peers + 2)
    for copy in tables:
        copy.start()
    for c in range(PARTS):
        to_mate(c).start()
    for c in range(PARTS):
        to_near(c).start()

    first_expert = z * peers

    def masks_of(s):
        routes = routes_ref[...] if s == 0 else routes_far[s - 1]
        return slot_masks(routes, first_expert, count, peers, capacity)

    def picks_of(masks):
        return jnp.where(masks[0] | masks[1], 1.0, 0.0).astype(jnp.bfloat16)

    def combines(s, masks):
        weights = weights_ref[...] if s == 0 else weights_far[s - 1]
        combine = (
            jnp.where(masks[0], weights[0:1, :], 0.0) + jnp.where(masks[1], weights[1:2, :], 0.0)
        ).T
        high = combine.astype(jnp.bfloat16)
        return high, (combine - high.astype(jnp.float32)).astype(jnp.bfloat16)

    def spread(s, c, picks):
        cols = slice(c * span, (c + 1) * span)
        source = xin_ref[:, cols] if s == 0 else xin_far[s - 1, :, cols]
        buffer[s, :, cols] = jnp.dot(picks, source, preferred_element_type=jnp.float32).astype(
            jnp.bfloat16
        )
        each(lambda i: outgoing(s, c, i).start())
        own_in(s, c).start()

    def combined(s, c, pair):
        block = returned[s, :, c * span : (c + 1) * span]
        return jnp.dot(pair[0], block, preferred_element_type=jnp.float32) + jnp.dot(
            pair[1], block, preferred_element_type=jnp.float32
        )

    def compute(s):
        for c in range(PARTS):
            own_in(s, c).wait()
            each(lambda i, c=c: outgoing(s, c, i).wait_recv())

        def make_hidden(j, carry):
            cols = pl.ds(pl.multiple_of(j * 256, 256), 256)
            gate_part = jnp.dot(received[s], gate[:, cols], preferred_element_type=jnp.float32)
            up_part = jnp.dot(received[s], up[:, cols], preferred_element_type=jnp.float32)
            hidden[:, cols] = (jax.nn.silu(gate_part) * up_part).astype(jnp.bfloat16)
            return carry

        lax.fori_loop(0, width // 256, make_hidden, 0)
        for c in range(PARTS):
            cols = slice(c * span, (c + 1) * span)
            results[s, :, cols] = jnp.dot(
                hidden[...], down[:, cols], preferred_element_type=jnp.float32
            ).astype(jnp.bfloat16)
            own_out(s, c).start()
            each(lambda i, c=c: returning(s, c, i).start())

    def returned_here(s, c):
        own_out(s, c).wait()
        each(lambda i: returning(s, c, i).wait_recv())

    def send_sums(s, pair):
        for c in range(PARTS):
            cols = slice(c * span, (c + 1) * span)
            returned_here(s, c)
            total = combined(s, c, pair)
            if s == 1:
                partial[s - 1, :, cols] = total.astype(jnp.bfloat16)
            else:

                @pl.when(inside == 0)
                def _(total=total, cols=cols):
                    partial[s - 1, :, cols] = total.astype(jnp.bfloat16)

                @pl.when(inside == 1)
                def _(total=total, cols=cols, c=c):
                    sum_here(s, c)
                    partial[s - 1, :, cols] = (
                        total + inbox[s, :, cols].astype(jnp.float32)
                    ).astype(jnp.bfloat16)

            sum_out(s, c).start()

    def relays(s):
        @pl.when(inside == 1)
        def _():
            for c in range(PARTS):
                line_here(s, c)
                relay(s, c).start()

    def dispatch(s, picks):
        for c in range(PARTS):
            if s in (2, 3):

                @pl.when(inside == 0)
                def _(c=c):
                    line_here(s, c)
            else:
                line_here(s, c)
            spread(s, c, picks)

    masks = masks_of(0)
    picks = picks_of(masks)
    for c in range(PARTS):
        spread(0, c, picks)
    pairs = [combines(0, masks)]
    later = []
    for s in (1, 2, 3):
        tables_here(s)
        masks = masks_of(s)
        later.append(picks_of(masks))
        pairs.append(combines(s, masks))
    for load in loads:
        load.wait()

    compute(0)
    relays(2)
    dispatch(1, later[0])
    compute(1)
    relays(3)
    dispatch(2, later[1])
    send_sums(1, pairs[1])
    compute(2)
    dispatch(3, later[2])
    send_sums(2, pairs[2])
    compute(3)
    for c in range(PARTS):
        cols = slice(c * span, (c + 1) * span)
        returned_here(0, c)
        sum_here(0, c)
        near_sum[:, cols] = (
            mid_ref[:, cols].astype(jnp.float32)
            + combined(0, c, pairs[0])
            + inbox[0, :, cols].astype(jnp.float32)
        )
    send_sums(3, pairs[3])
    for c in range(PARTS):
        cols = slice(c * span, (c + 1) * span)
        sum_here(1, c)
        out_ref[:, cols] = (near_sum[:, cols] + inbox[1, :, cols].astype(jnp.float32)).astype(
            jnp.bfloat16
        )

    for copy in tables:
        copy.wait_send()
    for c in range(PARTS):
        to_mate(c).wait_send()
        to_near(c).wait_send()
        for s in (1, 2, 3):
            sum_out(s, c).wait_send()

    @pl.when(inside == 1)
    def _():
        for c in range(PARTS):
            relay(2, c).wait_send()
            relay(3, c).wait_send()

    def drain(i):
        for s in range(LINE):
            for c in range(PARTS):
                outgoing(s, c, i).wait_send()
                returning(s, c, i).wait_send()

    each(drain)


def kernels_on_device(
    residual,
    query_maps,
    key_maps,
    value_rows,
    lambdas,
    head_gain,
    out_weight,
    ffn_gain,
    routes,
    route_weights,
    expert_gate,
    expert_up,
    expert_down,
):
    count_sp = lax.axis_size("sp")
    count_dp = lax.axis_size("dp")
    experts_all = count_sp * count_dp
    rows = residual.shape[1]
    capacity = max(2, 4 * rows // experts_all)
    if capacity % 16 or count_sp % LINE:
        return on_device(
            residual,
            query_maps,
            key_maps,
            value_rows,
            lambdas,
            head_gain,
            out_weight,
            ffn_gain,
            routes,
            route_weights,
            expert_gate,
            expert_up,
            expert_down,
        )
    heads_here = HEADS // count_sp
    peers = experts_all // LINE
    slots = peers * capacity
    vmem = pl.BlockSpec(memory_space=pltpu.VMEM)
    hbm = pl.BlockSpec(memory_space=pl.ANY)
    dma = pltpu.SemaphoreType.DMA
    bf16 = jnp.bfloat16
    length = rows * count_sp
    middle, expert_input = pl.pallas_call(
        functools.partial(mixer_kernel, count_sp),
        out_shape=(
            jax.ShapeDtypeStruct((rows, D), bf16),
            jax.ShapeDtypeStruct((rows, D), bf16),
        ),
        in_specs=[pl.BlockSpec(memory_space=pltpu.SMEM), hbm, hbm, hbm, vmem, vmem, hbm, vmem],
        out_specs=(vmem, vmem),
        scratch_shapes=[
            pltpu.VMEM((heads_here, length, VD), bf16),
            pltpu.VMEM((heads_here, length, VD), bf16),
            pltpu.VMEM((heads_here, length, VD), bf16),
            pltpu.VMEM((heads_here, length, VD), bf16),
            pltpu.VMEM((rows, HEADS * VD), bf16),
            pltpu.VMEM(out_weight.shape, bf16),
            dma((3, heads_here, count_sp)),
            dma((3, heads_here, count_sp)),
            dma((heads_here, count_sp)),
            dma((heads_here, count_sp)),
            dma((3, heads_here)),
            dma,
        ],
        compiler_params=pltpu.CompilerParams(
            collective_id=0, has_side_effects=True, vmem_limit_bytes=VMEM_LIMIT
        ),
    )(
        lambdas,
        query_maps[0],
        key_maps[0],
        value_rows[0],
        residual[0],
        head_gain.reshape(HEADS, VD),
        out_weight,
        ffn_gain.reshape(1, D),
    )
    width = expert_gate.shape[2]
    out = pl.pallas_call(
        functools.partial(experts_kernel, count_sp, count_dp, capacity),
        out_shape=jax.ShapeDtypeStruct((rows, D), bf16),
        in_specs=[vmem, vmem, vmem, vmem, hbm, hbm, hbm],
        out_specs=vmem,
        scratch_shapes=[
            pltpu.VMEM((LINE - 1, routes.shape[2], rows), jnp.int32),
            pltpu.VMEM((LINE - 1, routes.shape[2], rows), jnp.float32),
            pltpu.VMEM((LINE - 1, rows, D), bf16),
            pltpu.VMEM((LINE - 1, rows, D), bf16),
            pltpu.VMEM((LINE, rows, D), bf16),
            pltpu.VMEM((rows, D), jnp.float32),
            pltpu.VMEM((LINE, slots, D), bf16),
            pltpu.VMEM((LINE, slots, D), bf16),
            pltpu.VMEM((LINE, slots, D), bf16),
            pltpu.VMEM((LINE, slots, D), bf16),
            pltpu.VMEM((D, width), bf16),
            pltpu.VMEM((D, width), bf16),
            pltpu.VMEM((width, D), bf16),
            pltpu.VMEM((slots, width), bf16),
            dma((LINE - 1, 2)),
            dma((LINE - 1, 2)),
            dma((LINE, PARTS)),
            dma((LINE - 1, PARTS)),
            dma((LINE - 1, PARTS)),
            dma((LINE, PARTS)),
            dma((LINE, PARTS, peers)),
            dma((LINE, PARTS, peers)),
            dma((LINE, PARTS, peers)),
            dma((LINE, PARTS, peers)),
            dma((2, LINE, PARTS)),
            dma((3,)),
        ],
        compiler_params=pltpu.CompilerParams(
            collective_id=1, has_side_effects=True, vmem_limit_bytes=VMEM_LIMIT
        ),
    )(
        expert_input,
        middle,
        routes[0].T,
        route_weights[0].T,
        expert_gate[0],
        expert_up[0],
        expert_down[0],
    )
    return out[None]


def solution(mesh):
    return jax.shard_map(
        kernels_on_device,
        mesh=mesh,
        in_specs=(
            P("dp", "sp", None),
            P("dp", "sp", None),
            P("dp", "sp", None),
            P("dp", "sp", None),
            P(),
            P(),
            P(),
            P(),
            P("dp", "sp", None),
            P("dp", "sp", None),
            P(("sp", "dp"), None, None),
            P(("sp", "dp"), None, None),
            P(("sp", "dp"), None, None),
        ),
        out_specs=P("dp", "sp", None),
        check_vma=False,
    )
```

```python
import functools
import math

import jax
import jax.numpy as jnp
from jax import lax
from jax.experimental import pallas as pl
from jax.experimental.pallas import tpu as pltpu
from jax.sharding import PartitionSpec as P

D = 2048
HEADS = 16
HD = 64
VD = 128


eps = 1e-06


def attend_head(query_head, key_head, value_head, lam_head, gain_head):
    length = query_head.shape[0]
    block_rows = min(512, length)
    count_blocks = length // block_rows
    scaling = query_head.shape[-1] ** (-0.5)
    query_blocks = query_head.reshape(count_blocks, block_rows, 2, query_head.shape[-1])

    def one_block(query_block):
        scores = (
            jnp.einsum("qmd,kmd->mqk", query_block, key_head, preferred_element_type=jnp.float32)
            * scaling
        )
        probabilities = jax.nn.softmax(scores, axis=-1)
        mixed_map = (probabilities[0] - lam_head * probabilities[1]).astype(jnp.bfloat16)
        head_out = jnp.dot(mixed_map, value_head, preferred_element_type=jnp.float32)
        normed = head_out * lax.rsqrt(jnp.mean(head_out * head_out, axis=-1, keepdims=True) + eps)
        return (normed * gain_head * 0.8).astype(jnp.bfloat16)

    return lax.map(one_block, query_blocks).reshape(length, value_head.shape[-1])


def on_device(
    residual,
    query_maps,
    key_maps,
    value_rows,
    lambdas,
    head_gain,
    out_weight,
    ffn_gain,
    routes,
    route_weights,
    expert_gate,
    expert_up,
    expert_down,
):
    count_sp = lax.axis_size("sp")
    count_dp = lax.axis_size("dp")
    heads_here = HEADS // count_sp
    queries, keys_all, values_all = (
        lax.all_to_all(query_maps, "sp", split_axis=2, concat_axis=1, tiled=True),
        lax.all_to_all(key_maps, "sp", split_axis=2, concat_axis=1, tiled=True),
        lax.all_to_all(value_rows, "sp", split_axis=2, concat_axis=1, tiled=True),
    )
    first_head = lax.axis_index("sp") * heads_here
    lam_here = lax.dynamic_slice_in_dim(lambdas, first_head, heads_here)
    gain_here = lax.dynamic_slice_in_dim(head_gain, first_head * VD, heads_here * VD)
    outputs = []
    for head_index in range(heads_here):
        query_head = queries[0, :, head_index * 2 * HD : (head_index + 1) * 2 * HD].reshape(
            -1, 2, HD
        )
        key_head = keys_all[0, :, head_index * 2 * HD : (head_index + 1) * 2 * HD].reshape(
            -1, 2, HD
        )
        value_head = values_all[0, :, head_index * VD : (head_index + 1) * VD]
        gain_head = gain_here[head_index * VD : (head_index + 1) * VD]
        outputs.append(
            attend_head(query_head, key_head, value_head, lam_here[head_index], gain_head)
        )
    attended = jnp.concatenate(outputs, axis=1)[None]
    returned_heads = lax.all_to_all(attended, "sp", split_axis=1, concat_axis=2, tiled=True)
    projected = jnp.dot(returned_heads[0], out_weight, preferred_element_type=jnp.float32)
    residual_mid = (residual[0].astype(jnp.float32) + projected).astype(jnp.bfloat16)
    middle = residual_mid.astype(jnp.float32)
    expert_input = (
        middle * lax.rsqrt(jnp.mean(middle * middle, axis=-1, keepdims=True) + eps) * ffn_gain
    ).astype(jnp.bfloat16)
    tok_rows = residual.shape[1]
    experts_all = count_sp * count_dp
    capacity = max(2, 4 * tok_rows // experts_all)
    flat_routes = routes[0].reshape(-1)
    flat_weights = route_weights[0].reshape(-1)
    onehot = (flat_routes[:, None] == jnp.arange(experts_all, dtype=jnp.int32)[None, :]).astype(
        jnp.int32
    )
    before = jnp.cumsum(onehot, axis=0) - onehot
    rank_of = jnp.sum(before * onehot, axis=1)
    slot = flat_routes * capacity + rank_of
    token_of = jnp.arange(flat_routes.shape[0], dtype=jnp.int32) // routes.shape[2]
    slot_token = jnp.full((experts_all * capacity,), tok_rows, jnp.int32).at[slot].set(token_of)
    padded_input = jnp.concatenate([expert_input, jnp.zeros((1, D), jnp.bfloat16)], axis=0)
    buffer = padded_input[slot_token].reshape(experts_all, capacity, D)
    received = lax.all_to_all(buffer, ("sp", "dp"), split_axis=0, concat_axis=0, tiled=True)
    row_block = received.reshape(-1, D)
    gate_part = jnp.dot(row_block, expert_gate[0], preferred_element_type=jnp.float32)
    up_part = jnp.dot(row_block, expert_up[0], preferred_element_type=jnp.float32)
    hidden = (jax.nn.silu(gate_part) * up_part).astype(jnp.bfloat16)
    expert_out = jnp.dot(hidden, expert_down[0], preferred_element_type=jnp.float32).astype(
        jnp.bfloat16
    )
    returned = lax.all_to_all(
        expert_out.reshape(received.shape), ("sp", "dp"), split_axis=0, concat_axis=0, tiled=True
    )
    picked = returned.reshape(experts_all * capacity, D)[slot]
    weighted = (picked.astype(jnp.float32) * flat_weights[:, None]).reshape(
        tok_rows, routes.shape[2], D
    )
    layer_out = (middle + jnp.sum(weighted, axis=1)).astype(jnp.bfloat16)
    return layer_out[None]


MESH = pl.DeviceIdType.MESH
VMEM_LIMIT = 60 * 1024 * 1024


def slot_masks(routes, first_expert, experts_all, experts_here, capacity):
    rows = routes.shape[1]
    first, second = routes[0:1, :], routes[1:2, :]
    experts = lax.broadcasted_iota(jnp.int32, (experts_all, rows), 0)
    named_first, named_second = experts == first, experts == second
    named = jnp.where(named_first | named_second, 1.0, 0.0).astype(jnp.bfloat16)
    earlier = lax.broadcasted_iota(jnp.int32, (rows, rows), 0) < lax.broadcasted_iota(
        jnp.int32, (rows, rows), 1
    )
    before = jnp.dot(
        named, jnp.where(earlier, 1.0, 0.0).astype(jnp.bfloat16), preferred_element_type=jnp.float32
    )
    slots = lax.broadcasted_iota(jnp.int32, (experts_here * capacity, rows), 0)
    masks = []
    for route, chosen in ((first, named_first), (second, named_second)):
        rank = jnp.sum(jnp.where(chosen, before, 0.0), axis=0, keepdims=True).astype(jnp.int32)
        masks.append(slots == (route - first_expert) * capacity + rank)
    return masks


PARTS = 4
LINE = 4


def layer_kernel(
    count_sp,
    count_dp,
    capacity,
    lam_ref,
    q_ref,
    k_ref,
    v_ref,
    residual_ref,
    gain_ref,
    ow_hbm,
    fgain_ref,
    routes_ref,
    weights_ref,
    gate_hbm,
    up_hbm,
    down_hbm,
    out_ref,
    staged,
    qh,
    kh,
    vh,
    outs,
    att,
    ow,
    mid,
    xin,
    routes_far,
    weights_far,
    picks,
    shares,
    far,
    partial,
    inbox,
    total,
    buffer,
    received,
    results,
    returned,
    far_buffer,
    far_received,
    far_results,
    far_returned,
    gate,
    up,
    down,
    hidden,
    send_sem,
    key_recv,
    query_recv,
    value_recv,
    back_send,
    back_recv,
    ow_sem,
    weight_sem,
    table_send,
    table_recv,
    far_send,
    far_recv,
    relay_send,
    sum_send,
    sum_recv,
    go_send,
    go_recv,
    ret_send,
    ret_recv,
    fgo_send,
    fgo_recv,
    fret_send,
    fret_recv,
    stage_sem,
):
    me_sp = lax.axis_index("sp")
    rows = q_ref.shape[0]
    heads_here = HEADS // count_sp
    sources = ((staged.at[0], kh), (staged.at[1], qh), (staged.at[2], vh))
    stages = [
        pltpu.make_async_copy(src, staged.at[t], stage_sem.at[t])
        for t, src in enumerate((k_ref, q_ref, v_ref))
    ]
    for t in (0, 2, 1):
        stages[t].start()

    count = count_sp * count_dp
    inner = count_sp // LINE
    half = count // 2
    plane = half // 2
    z, y = me_sp // inner, lax.rem(me_sp, inner)
    side = z // 2
    base = side * half
    me = me_sp * count_dp + lax.axis_index("dp") - base
    me_z, me_j = me // plane, lax.rem(me, plane)
    inside = (z * (LINE - 1 - z)) // 2
    gate_z = 1 - side
    mate_z = z + 1 - 2 * lax.rem(z, 2)
    near_z = 2 - side
    last_z = 3 - 3 * side
    width = gate.shape[1]
    span = D // PARTS

    def coords(p):
        return {"sp": (base + p) // count_dp, "dp": lax.rem(base + p, count_dp)}

    def on_line(other):
        return {"sp": other * inner + y}

    def peer(i):
        e = i + i // plane
        return lax.rem(me_z + 1 + e // plane, 2) * plane + lax.rem(me_j + e, plane)

    barrier = pltpu.get_barrier_semaphore()

    def greet(d, carry):
        pl.semaphore_signal(
            barrier, inc=1, device_id={"sp": lax.rem(me_sp + d, count_sp)}, device_id_type=MESH
        )
        return carry

    lax.fori_loop(1, count_sp, greet, 0)

    def greet_half(i, carry):
        pl.semaphore_signal(barrier, inc=1, device_id=coords(peer(i)), device_id_type=MESH)
        return carry

    lax.fori_loop(0, half - 1, greet_half, 0)

    my_rows = pl.ds(pl.multiple_of(me_sp * rows, rows), rows)

    def arrival(t, h, d):
        return (key_recv.at[h], query_recv.at[h, d], value_recv.at[h])[t]

    def local_copy(t, h):
        src, dst = sources[t]
        cols = pl.ds(pl.multiple_of((me_sp * heads_here + h) * VD, VD), VD)
        return pltpu.make_async_copy(src.at[:, cols], dst.at[h, my_rows, :], arrival(t, h, 0))

    def outgoing(t, h, d):
        src, dst = sources[t]
        to = lax.rem(me_sp + d, count_sp)
        cols = pl.ds(pl.multiple_of((to * heads_here + h) * VD, VD), VD)
        return pltpu.make_async_remote_copy(
            src_ref=src.at[:, cols],
            dst_ref=dst.at[h, my_rows, :],
            send_sem=send_sem,
            recv_sem=arrival(t, h, d),
            device_id={"sp": to},
            device_id_type=MESH,
        )

    def landed(ref, sem):
        pltpu.make_async_copy(ref, ref, sem).wait()

    def table(t, n, slot):
        src, dst = ((routes_ref, routes_far), (weights_ref, weights_far))[t]
        return pltpu.make_async_remote_copy(
            src_ref=src,
            dst_ref=dst.at[slot],
            send_sem=table_send.at[t, n],
            recv_sem=table_recv.at[slot, t],
            device_id=on_line((near_z, last_z)[n]),
            device_id_type=MESH,
        )

    weight_copy = pltpu.make_async_copy(ow_hbm, ow, ow_sem)
    loads = [
        pltpu.make_async_copy(src, dst, weight_sem.at[j])
        for j, (src, dst) in enumerate(((gate_hbm, gate), (up_hbm, up), (down_hbm, down)))
    ]

    pl.semaphore_wait(barrier, count_sp - 1 + half - 1)
    for h in range(heads_here):

        for t in (0, 2, 1):
            if h == 0:
                stages[t].wait()

            def start_all(i, carry, t=t, h=h):
                outgoing(t, h, 1 + lax.rem(i + count_sp // 2 - 1, count_sp - 1)).start()
                return carry

            lax.fori_loop(0, count_sp - 1, start_all, 0)
            local_copy(t, h).start()
    for n in range(2):
        for t in range(2):
            table(t, n, 1 - inside).start()
    weight_copy.start()
    for load in loads:
        load.start()

    def set_tables(slot, routes, weights):
        masks = slot_masks(routes, base, count, half, capacity)
        picks[slot] = jnp.where(masks[0] | masks[1], 1.0, 0.0).astype(jnp.bfloat16)
        combine = (
            jnp.where(masks[0], weights[0:1, :], 0.0) + jnp.where(masks[1], weights[1:2, :], 0.0)
        ).T
        high = combine.astype(jnp.bfloat16)
        shares[slot, 0] = high
        shares[slot, 1] = (combine - high.astype(jnp.float32)).astype(jnp.bfloat16)

    set_tables(0, routes_ref[...], weights_ref[...])

    def returning(h, p, d):
        dst_cols = pl.ds(pl.multiple_of((me_sp * heads_here + h) * VD, VD), VD)
        return pltpu.make_async_remote_copy(
            src_ref=outs.at[h, pl.ds(pl.multiple_of(p * rows, rows), rows), :],
            dst_ref=att.at[:, dst_cols],
            send_sem=back_send,
            recv_sem=back_recv,
            device_id={"sp": p},
            device_id_type=MESH,
        )

    factor = HD ** (-0.5) * math.log2(math.e)
    lanes = lax.broadcasted_iota(jnp.int32, (rows, VD), 1)
    for h in range(heads_here):
        with jax.named_scope("kv"):
            landed(kh.at[h], key_recv.at[h])
            landed(vh.at[h], value_recv.at[h])
        head = me_sp * heads_here + h
        lam = lam_ref[head]
        gain = gain_ref[pl.ds(head, 1), :]

        def attend(p, h=h, lam=lam, gain=gain):
            at = pl.ds(pl.multiple_of(p * rows, rows), rows)
            q = qh[h, at, :]
            zero = jnp.zeros_like(q)
            both = jnp.concatenate(
                [jnp.where(lanes < HD, q, zero), jnp.where(lanes < HD, zero, q)], axis=0
            )
            scores = lax.dot_general(
                both, kh[h], (((1,), (1,)), ((), ())), preferred_element_type=jnp.float32
            )
            top = jnp.max(scores, axis=1, keepdims=True)
            e = jnp.exp2((scores - top) * factor)
            norm = jnp.sum(e, axis=1, keepdims=True)
            norm_1, norm_2 = norm[:rows], norm[rows:]
            share = lam * norm_1 / norm_2
            mixed = (e[:rows] - share * e[rows:]).astype(jnp.bfloat16)
            head_out = jnp.dot(mixed, vh[h], preferred_element_type=jnp.float32) / norm_1
            normed = head_out * lax.rsqrt(
                jnp.mean(head_out * head_out, axis=-1, keepdims=True) + eps
            )
            return (normed * gain * 0.8).astype(jnp.bfloat16)

        def step(i, carry, h=h, attend=attend):
            d = 1 + lax.rem(i + count_sp // 2 - 1, count_sp - 1)
            p = lax.rem(me_sp + count_sp - d, count_sp)
            outgoing(1, h, d).wait_recv()
            outs[h, pl.ds(pl.multiple_of(p * rows, rows), rows), :] = attend(p)
            returning(h, p, d).start()
            return carry

        with jax.named_scope("steps"):
            lax.fori_loop(0, count_sp - 1, step, 0)
        local_copy(1, h).wait()
        with jax.named_scope("mine"):
            att[:, pl.ds(pl.multiple_of(head * VD, VD), VD)] = attend(me_sp)

    for slot in range(2):
        for t in range(2):
            table(t, 0, slot).wait_recv()
        set_tables(1 + slot, routes_far[slot], weights_far[slot])

    weight_copy.wait()
    others = (count_sp - 1) * heads_here * VD
    with jax.named_scope("back"):
        landed(att.at[:, pl.ds(0, others)], back_recv)

    tile = 512
    square = jnp.zeros((rows, 1), jnp.float32)
    for j in range(D // tile):
        cols = slice(j * tile, (j + 1) * tile)
        projected = jnp.dot(att[...], ow[:, cols], preferred_element_type=jnp.float32)
        middle = (residual_ref[:, cols].astype(jnp.float32) + projected).astype(jnp.bfloat16)
        mid[:, cols] = middle
        wide = middle.astype(jnp.float32)
        square = square + jnp.sum(wide * wide, axis=1, keepdims=True)
    scale = lax.rsqrt(square / D + eps)
    xin[...] = (mid[...].astype(jnp.float32) * scale * fgain_ref[...]).astype(jnp.bfloat16)

    def rows_of(i):
        return pl.ds(pl.multiple_of(i * capacity, capacity), capacity)

    def part(c):
        return pl.ds(c * span, span)

    def remote(src, dst, sent, got, target):
        return pltpu.make_async_remote_copy(
            src_ref=src,
            dst_ref=dst,
            send_sem=sent,
            recv_sem=got,
            device_id=target,
            device_id_type=MESH,
        )

    def cross(c):
        slot = 1 - inside
        return remote(
            xin.at[:, part(c)],
            far.at[slot, :, part(c)],
            far_send,
            far_recv.at[slot, c],
            on_line(near_z),
        )

    def crossed(k, c):
        landed(far.at[k, :, part(c)], far_recv.at[k, c])

    def go(c, q, own):
        return remote(
            buffer.at[rows_of(q), part(c)],
            received.at[rows_of(me), part(c)],
            go_send,
            go_recv.at[own, c],
            coords(q),
        )

    def ret(c, q):
        return remote(
            results.at[rows_of(q), part(c)],
            returned.at[rows_of(me), part(c)],
            ret_send,
            ret_recv.at[c],
            coords(q),
        )

    def relay(k, c):
        held = far.at[k, :, part(c)]
        return remote(held, held, relay_send, far_recv.at[k, c], on_line(mate_z))

    def far_go(k, c, j):
        return remote(
            far_buffer.at[k, rows_of(j), part(c)],
            far_received.at[k, rows_of(me_j), part(c)],
            fgo_send,
            fgo_recv.at[k, c],
            coords(me_z * plane + j),
        )

    def far_ret(k, c, j):
        return remote(
            far_results.at[k, rows_of(j), part(c)],
            far_returned.at[k, rows_of(me), part(c)],
            fret_send,
            fret_recv.at[k, c],
            coords(gate_z * plane + j),
        )

    def sum_out(k, c):
        return remote(
            partial.at[k, :, part(c)],
            inbox.at[:, part(c)],
            sum_send,
            sum_recv.at[c],
            on_line(near_z if k == 0 else last_z),
        )

    def sum_here(c):
        landed(inbox.at[:, part(c)], sum_recv.at[c])

    def own_in(c):
        return pltpu.make_async_copy(
            buffer.at[rows_of(me), part(c)], received.at[rows_of(me), part(c)], go_recv.at[1, c]
        )

    def own_out(c):
        return pltpu.make_async_copy(
            results.at[rows_of(me), part(c)], returned.at[rows_of(me), part(c)], ret_recv.at[c]
        )

    def far_own_in(k, c):
        return pltpu.make_async_copy(
            far_buffer.at[k, rows_of(me_j), part(c)],
            far_received.at[k, rows_of(me_j), part(c)],
            fgo_recv.at[k, c],
        )

    def far_own_out(k, c):
        return pltpu.make_async_copy(
            far_results.at[k, rows_of(me_j), part(c)],
            far_returned.at[k, rows_of(me), part(c)],
            fret_recv.at[k, c],
        )

    def each(first, last, do):
        def loop(i, carry):
            do(i)
            return carry

        lax.fori_loop(first, last, loop, 0)

    def peers(do):
        each(0, half - 1, lambda i: do(peer(i)))

    def mates(do):
        each(1, plane, lambda i: do(lax.rem(me_j + i, plane)))

    def cut(c):
        return slice(c * span, (c + 1) * span)

    def spread(c):
        buffer[:, cut(c)] = jnp.dot(
            picks[0], xin[:, cut(c)], preferred_element_type=jnp.float32
        ).astype(jnp.bfloat16)
        mates(lambda j: go(c, me_z * plane + j, 1).start())
        own_in(c).start()

    def across(c):
        far_z = 1 - me_z
        each(0, plane, lambda i: go(c, far_z * plane + lax.rem(me_j + i, plane), 0).start())

    plane_rows = plane * capacity
    my_plane = pl.ds(pl.multiple_of(me_z * plane_rows, plane_rows), plane_rows)

    def far_spread(k, relaying):
        for c in range(PARTS):
            crossed(k, c)
            if relaying:
                relay(k, c).start()
            far_buffer[k, :, cut(c)] = jnp.dot(
                picks[1 + k, my_plane], far[k, :, cut(c)], preferred_element_type=jnp.float32
            ).astype(jnp.bfloat16)
            mates(lambda j, c=c: far_go(k, c, j).start())
            far_own_in(k, c).start()

    def expert(source, target, send):
        def make_hidden(j, carry):
            cols = pl.ds(pl.multiple_of(j * 256, 256), 256)
            gate_part = jnp.dot(source[...], gate[:, cols], preferred_element_type=jnp.float32)
            up_part = jnp.dot(source[...], up[:, cols], preferred_element_type=jnp.float32)
            hidden[:, cols] = (jax.nn.silu(gate_part) * up_part).astype(jnp.bfloat16)
            return carry

        lax.fori_loop(0, width // 256, make_hidden, 0)
        for c in range(PARTS):
            target[:, cut(c)] = jnp.dot(
                hidden[...], down[:, cut(c)], preferred_element_type=jnp.float32
            ).astype(jnp.bfloat16)
            send(c)

    def near_return(c, own):
        which = me_z if own else 1 - me_z
        if own:
            own_out(c).start()
            mates(lambda j: ret(c, which * plane + j).start())
        else:
            each(0, plane, lambda i: ret(c, which * plane + lax.rem(me_j + i, plane)).start())

    def near_batch(own, later=False):
        which = me_z if own else 1 - me_z
        at = pl.ds(pl.multiple_of(which * plane_rows, plane_rows), plane_rows)
        for c in range(PARTS):
            landed(received.at[at, part(c)], go_recv.at[1 if own else 0, c])

        def send(c):
            if not later:
                near_return(c, own)

        expert(received.at[at], results.at[at], send)

    def far_batch(k, inner_side):
        for c in range(PARTS):
            landed(far_received.at[k, :, part(c)], fgo_recv.at[k, c])

        def send(c):
            if inner_side:
                far_own_out(k, c).start()
            else:
                far_ret(k, c, me_j).start()
            mates(lambda j: far_ret(k, c, j).start())

        expert(far_received.at[k], far_results.at[k], send)

    def summed(slot, block):
        return jnp.dot(shares[slot, 0], block, preferred_element_type=jnp.float32) + jnp.dot(
            shares[slot, 1], block, preferred_element_type=jnp.float32
        )

    def far_sums(k):
        for c in range(PARTS):
            landed(far_returned.at[k, :, part(c)], fret_recv.at[k, c])
            partial[k, :, cut(c)] = summed(1 + k, far_returned[k, :, cut(c)]).astype(jnp.bfloat16)
            sum_out(k, c).start()

    def near_sums():
        for c in range(PARTS):
            landed(returned.at[:, part(c)], ret_recv.at[c])
            total[:, cut(c)] = mid[:, cut(c)].astype(jnp.float32) + summed(0, returned[:, cut(c)])

    for load in loads:
        load.wait()

    @pl.when(inside == 1)
    def _():
        with jax.named_scope("go"):
            for c in range(PARTS):
                spread(c)
                cross(c).start()
        with jax.named_scope("d1"):
            far_spread(0, True)
        with jax.named_scope("own"):
            near_batch(True)
        with jax.named_scope("d2"):
            far_spread(1, True)
        with jax.named_scope("ac"):
            for c in range(PARTS):
                across(c)
        with jax.named_scope("mate"):
            near_batch(False, True)
        with jax.named_scope("rt"):
            for c in range(PARTS):
                near_return(c, False)
        with jax.named_scope("b1"):
            far_batch(0, True)
        with jax.named_scope("b2"):
            far_batch(1, True)
        with jax.named_scope("s1"):
            far_sums(0)
        with jax.named_scope("s2"):
            far_sums(1)
        with jax.named_scope("near"):
            near_sums()

    @pl.when(inside == 0)
    def _():
        with jax.named_scope("go"):
            for c in range(PARTS):
                spread(c)
                across(c)
            for c in range(PARTS):
                cross(c).start()
        with jax.named_scope("own"):
            near_batch(True)
        with jax.named_scope("d1"):
            far_spread(0, False)
        with jax.named_scope("b1"):
            far_batch(0, False)
        with jax.named_scope("d2"):
            far_spread(1, False)
        with jax.named_scope("b2"):
            far_batch(1, False)
        with jax.named_scope("mate"):
            near_batch(False)
        with jax.named_scope("near"):
            near_sums()

    with jax.named_scope("end"):
        for c in range(PARTS):
            sum_here(c)
            out_ref[:, cut(c)] = (total[:, cut(c)] + inbox[:, cut(c)].astype(jnp.float32)).astype(
                jnp.bfloat16
            )

    with jax.named_scope("drain"):
        for n in range(2):
            for t in range(2):
                table(t, n, 1 - inside).wait_send()

        def gone(ref, sem):
            remote(ref, ref, sem, sum_recv.at[0], on_line(near_z)).wait_send()

        gone(staged.at[:, :, pl.ds(0, others)], send_sem)
        gone(outs.at[:, pl.ds(0, (count_sp - 1) * rows), :], back_send)
        gone(buffer.at[pl.ds(0, (half - 1) * capacity)], go_send)
        gone(results.at[pl.ds(0, (half - 1) * capacity)], ret_send)
        gone(far_buffer.at[:, pl.ds(0, (plane - 1) * capacity)], fgo_send)
        gone(xin, far_send)

        @pl.when(inside == 0)
        def _():
            gone(far_results, fret_send)

        @pl.when(inside == 1)
        def _():
            gone(far_results.at[:, pl.ds(0, (plane - 1) * capacity)], fret_send)
            gone(far, relay_send)
            gone(partial, sum_send)


def kernels_on_device(
    residual,
    query_maps,
    key_maps,
    value_rows,
    lambdas,
    head_gain,
    out_weight,
    ffn_gain,
    routes,
    route_weights,
    expert_gate,
    expert_up,
    expert_down,
):
    count_sp = lax.axis_size("sp")
    count_dp = lax.axis_size("dp")
    experts_all = count_sp * count_dp
    rows = residual.shape[1]
    capacity = max(2, 4 * rows // experts_all)
    if capacity % 16 or count_sp % LINE:
        return on_device(
            residual,
            query_maps,
            key_maps,
            value_rows,
            lambdas,
            head_gain,
            out_weight,
            ffn_gain,
            routes,
            route_weights,
            expert_gate,
            expert_up,
            expert_down,
        )
    heads_here = HEADS // count_sp
    half = experts_all // 2
    plane = half // 2
    slots = half * capacity
    vmem = pl.BlockSpec(memory_space=pltpu.VMEM)
    hbm = pl.BlockSpec(memory_space=pl.ANY)
    dma = pltpu.SemaphoreType.DMA
    bf16, f32 = jnp.bfloat16, jnp.float32
    length = rows * count_sp
    width = expert_gate.shape[2]
    top = routes.shape[2]
    out = pl.pallas_call(
        functools.partial(layer_kernel, count_sp, count_dp, capacity),
        out_shape=jax.ShapeDtypeStruct((rows, D), bf16),
        in_specs=[pl.BlockSpec(memory_space=pltpu.SMEM), hbm, hbm, hbm, vmem, vmem, hbm, vmem]
        + [vmem, vmem, hbm, hbm, hbm],
        out_specs=vmem,
        scratch_shapes=[
            pltpu.VMEM((3, rows, D), bf16),
            pltpu.VMEM((heads_here, length, VD), bf16),
            pltpu.VMEM((heads_here, length, VD), bf16),
            pltpu.VMEM((heads_here, length, VD), bf16),
            pltpu.VMEM((heads_here, length, VD), bf16),
            pltpu.VMEM((rows, HEADS * VD), bf16),
            pltpu.VMEM(out_weight.shape, bf16),
            pltpu.VMEM((rows, D), bf16),
            pltpu.VMEM((rows, D), bf16),
            pltpu.VMEM((2, top, rows), jnp.int32),
            pltpu.VMEM((2, top, rows), f32),
            pltpu.VMEM((3, slots, rows), bf16),
            pltpu.VMEM((3, 2, rows, slots), bf16),
            pltpu.VMEM((2, rows, D), bf16),
            pltpu.VMEM((2, rows, D), bf16),
            pltpu.VMEM((rows, D), bf16),
            pltpu.VMEM((rows, D), f32),
            pltpu.VMEM((slots, D), bf16),
            pltpu.VMEM((slots, D), bf16),
            pltpu.VMEM((slots, D), bf16),
            pltpu.VMEM((slots, D), bf16),
            pltpu.VMEM((2, slots // 2, D), bf16),
            pltpu.VMEM((2, slots // 2, D), bf16),
            pltpu.VMEM((2, slots // 2, D), bf16),
            pltpu.VMEM((2, slots, D), bf16),
            pltpu.VMEM((D, width), bf16),
            pltpu.VMEM((D, width), bf16),
            pltpu.VMEM((width, D), bf16),
            pltpu.VMEM((slots // 2, width), bf16),
            dma,
            dma((heads_here,)),
            dma((heads_here, count_sp)),
            dma((heads_here,)),
            dma,
            dma,
            dma,
            dma((3,)),
            dma((2, 2)),
            dma((2, 2)),
            dma,
            dma((2, PARTS)),
            dma,
            dma,
            dma((PARTS,)),
            dma,
            dma((2, PARTS)),
            dma,
            dma((PARTS,)),
            dma,
            dma((2, PARTS)),
            dma,
            dma((2, PARTS)),
            dma((3,)),
        ],
        compiler_params=pltpu.CompilerParams(
            collective_id=0, has_side_effects=True, vmem_limit_bytes=VMEM_LIMIT
        ),
    )(
        lambdas,
        query_maps[0],
        key_maps[0],
        value_rows[0],
        residual[0],
        head_gain.reshape(HEADS, VD),
        out_weight,
        ffn_gain.reshape(1, D),
        routes[0].T,
        route_weights[0].T,
        expert_gate[0],
        expert_up[0],
        expert_down[0],
    )
    return out[None]


def solution(mesh):
    return jax.shard_map(
        kernels_on_device,
        mesh=mesh,
        in_specs=(
            P("dp", "sp", None),
            P("dp", "sp", None),
            P("dp", "sp", None),
            P("dp", "sp", None),
            P(),
            P(),
            P(),
            P(),
            P("dp", "sp", None),
            P("dp", "sp", None),
            P(("sp", "dp"), None, None),
            P(("sp", "dp"), None, None),
            P(("sp", "dp"), None, None),
        ),
        out_specs=P("dp", "sp", None),
        check_vma=False,
    )
```

```python
import functools
import math

import jax
import jax.numpy as jnp
from jax import lax
from jax.experimental import pallas as pl
from jax.experimental.pallas import tpu as pltpu
from jax.sharding import PartitionSpec as P

D = 2048
HEADS = 16
HD = 64
VD = 128


eps = 1e-06


def attend_head(query_head, key_head, value_head, lam_head, gain_head):
    length = query_head.shape[0]
    block_rows = min(512, length)
    count_blocks = length // block_rows
    scaling = query_head.shape[-1] ** (-0.5)
    query_blocks = query_head.reshape(count_blocks, block_rows, 2, query_head.shape[-1])

    def one_block(query_block):
        scores = (
            jnp.einsum("qmd,kmd->mqk", query_block, key_head, preferred_element_type=jnp.float32)
            * scaling
        )
        probabilities = jax.nn.softmax(scores, axis=-1)
        mixed_map = (probabilities[0] - lam_head * probabilities[1]).astype(jnp.bfloat16)
        head_out = jnp.dot(mixed_map, value_head, preferred_element_type=jnp.float32)
        normed = head_out * lax.rsqrt(jnp.mean(head_out * head_out, axis=-1, keepdims=True) + eps)
        return (normed * gain_head * 0.8).astype(jnp.bfloat16)

    return lax.map(one_block, query_blocks).reshape(length, value_head.shape[-1])


def on_device(
    residual,
    query_maps,
    key_maps,
    value_rows,
    lambdas,
    head_gain,
    out_weight,
    ffn_gain,
    routes,
    route_weights,
    expert_gate,
    expert_up,
    expert_down,
):
    count_sp = lax.axis_size("sp")
    count_dp = lax.axis_size("dp")
    heads_here = HEADS // count_sp
    queries, keys_all, values_all = (
        lax.all_to_all(query_maps, "sp", split_axis=2, concat_axis=1, tiled=True),
        lax.all_to_all(key_maps, "sp", split_axis=2, concat_axis=1, tiled=True),
        lax.all_to_all(value_rows, "sp", split_axis=2, concat_axis=1, tiled=True),
    )
    first_head = lax.axis_index("sp") * heads_here
    lam_here = lax.dynamic_slice_in_dim(lambdas, first_head, heads_here)
    gain_here = lax.dynamic_slice_in_dim(head_gain, first_head * VD, heads_here * VD)
    outputs = []
    for head_index in range(heads_here):
        query_head = queries[0, :, head_index * 2 * HD : (head_index + 1) * 2 * HD].reshape(
            -1, 2, HD
        )
        key_head = keys_all[0, :, head_index * 2 * HD : (head_index + 1) * 2 * HD].reshape(
            -1, 2, HD
        )
        value_head = values_all[0, :, head_index * VD : (head_index + 1) * VD]
        gain_head = gain_here[head_index * VD : (head_index + 1) * VD]
        outputs.append(
            attend_head(query_head, key_head, value_head, lam_here[head_index], gain_head)
        )
    attended = jnp.concatenate(outputs, axis=1)[None]
    returned_heads = lax.all_to_all(attended, "sp", split_axis=1, concat_axis=2, tiled=True)
    projected = jnp.dot(returned_heads[0], out_weight, preferred_element_type=jnp.float32)
    residual_mid = (residual[0].astype(jnp.float32) + projected).astype(jnp.bfloat16)
    middle = residual_mid.astype(jnp.float32)
    expert_input = (
        middle * lax.rsqrt(jnp.mean(middle * middle, axis=-1, keepdims=True) + eps) * ffn_gain
    ).astype(jnp.bfloat16)
    tok_rows = residual.shape[1]
    experts_all = count_sp * count_dp
    capacity = max(2, 4 * tok_rows // experts_all)
    flat_routes = routes[0].reshape(-1)
    flat_weights = route_weights[0].reshape(-1)
    onehot = (flat_routes[:, None] == jnp.arange(experts_all, dtype=jnp.int32)[None, :]).astype(
        jnp.int32
    )
    before = jnp.cumsum(onehot, axis=0) - onehot
    rank_of = jnp.sum(before * onehot, axis=1)
    slot = flat_routes * capacity + rank_of
    token_of = jnp.arange(flat_routes.shape[0], dtype=jnp.int32) // routes.shape[2]
    slot_token = jnp.full((experts_all * capacity,), tok_rows, jnp.int32).at[slot].set(token_of)
    padded_input = jnp.concatenate([expert_input, jnp.zeros((1, D), jnp.bfloat16)], axis=0)
    buffer = padded_input[slot_token].reshape(experts_all, capacity, D)
    received = lax.all_to_all(buffer, ("sp", "dp"), split_axis=0, concat_axis=0, tiled=True)
    row_block = received.reshape(-1, D)
    gate_part = jnp.dot(row_block, expert_gate[0], preferred_element_type=jnp.float32)
    up_part = jnp.dot(row_block, expert_up[0], preferred_element_type=jnp.float32)
    hidden = (jax.nn.silu(gate_part) * up_part).astype(jnp.bfloat16)
    expert_out = jnp.dot(hidden, expert_down[0], preferred_element_type=jnp.float32).astype(
        jnp.bfloat16
    )
    returned = lax.all_to_all(
        expert_out.reshape(received.shape), ("sp", "dp"), split_axis=0, concat_axis=0, tiled=True
    )
    picked = returned.reshape(experts_all * capacity, D)[slot]
    weighted = (picked.astype(jnp.float32) * flat_weights[:, None]).reshape(
        tok_rows, routes.shape[2], D
    )
    layer_out = (middle + jnp.sum(weighted, axis=1)).astype(jnp.bfloat16)
    return layer_out[None]


MESH = pl.DeviceIdType.MESH
VMEM_LIMIT = 60 * 1024 * 1024


def slot_masks(routes, first_expert, experts_all, experts_here, capacity):
    rows = routes.shape[1]
    first, second = routes[0:1, :], routes[1:2, :]
    experts = lax.broadcasted_iota(jnp.int32, (experts_all, rows), 0)
    named_first, named_second = experts == first, experts == second
    named = jnp.where(named_first | named_second, 1.0, 0.0).astype(jnp.bfloat16)
    earlier = lax.broadcasted_iota(jnp.int32, (rows, rows), 0) < lax.broadcasted_iota(
        jnp.int32, (rows, rows), 1
    )
    before = jnp.dot(
        named, jnp.where(earlier, 1.0, 0.0).astype(jnp.bfloat16), preferred_element_type=jnp.float32
    )
    slots = lax.broadcasted_iota(jnp.int32, (experts_here * capacity, rows), 0)
    masks = []
    for route, chosen in ((first, named_first), (second, named_second)):
        rank = jnp.sum(jnp.where(chosen, before, 0.0), axis=0, keepdims=True).astype(jnp.int32)
        masks.append(slots == (route - first_expert) * capacity + rank)
    return masks


PARTS = 4
LINE = 4


def layer_kernel(
    count_sp,
    count_dp,
    capacity,
    lam_ref,
    q_ref,
    k_ref,
    v_ref,
    residual_ref,
    gain_ref,
    ow_hbm,
    fgain_ref,
    routes_ref,
    weights_ref,
    gate_hbm,
    up_hbm,
    down_hbm,
    out_ref,
    staged,
    qh,
    kh,
    vh,
    outs,
    att,
    ow,
    mid,
    xin,
    routes_far,
    weights_far,
    picks,
    shares,
    far,
    partial,
    inbox,
    total,
    buffer,
    received,
    results,
    returned,
    far_buffer,
    far_received,
    far_results,
    far_returned,
    gate,
    up,
    down,
    hidden,
    send_sem,
    key_recv,
    query_recv,
    value_recv,
    back_send,
    back_recv,
    ow_sem,
    weight_sem,
    table_send,
    table_recv,
    far_send,
    far_recv,
    relay_send,
    sum_send,
    sum_recv,
    go_send,
    go_recv,
    ret_send,
    ret_recv,
    fgo_send,
    fgo_recv,
    fret_send,
    fret_recv,
    stage_sem,
):
    me_sp = lax.axis_index("sp")
    rows = q_ref.shape[0]
    heads_here = HEADS // count_sp
    sources = ((staged.at[0], kh), (staged.at[1], qh), (staged.at[2], vh))
    stages = [
        pltpu.make_async_copy(src, staged.at[t], stage_sem.at[t])
        for t, src in enumerate((k_ref, q_ref, v_ref))
    ]
    for t in (0, 2, 1):
        stages[t].start()

    count = count_sp * count_dp
    inner = count_sp // LINE
    half = count // 2
    plane = half // 2
    z, y = me_sp // inner, lax.rem(me_sp, inner)
    side = z // 2
    base = side * half
    me = me_sp * count_dp + lax.axis_index("dp") - base
    me_z, me_j = me // plane, lax.rem(me, plane)
    inside = (z * (LINE - 1 - z)) // 2
    gate_z = 1 - side
    mate_z = z + 1 - 2 * lax.rem(z, 2)
    near_z = 2 - side
    last_z = 3 - 3 * side
    width = gate.shape[1]
    span = D // PARTS

    def coords(p):
        return {"sp": (base + p) // count_dp, "dp": lax.rem(base + p, count_dp)}

    def on_line(other):
        return {"sp": other * inner + y}

    def peer(i):
        e = i + i // plane
        return lax.rem(me_z + 1 + e // plane, 2) * plane + lax.rem(me_j + e, plane)

    barrier = pltpu.get_barrier_semaphore()

    def greet(d, carry):
        pl.semaphore_signal(
            barrier, inc=1, device_id={"sp": lax.rem(me_sp + d, count_sp)}, device_id_type=MESH
        )
        return carry

    lax.fori_loop(1, count_sp, greet, 0)

    def greet_half(i, carry):
        pl.semaphore_signal(barrier, inc=1, device_id=coords(peer(i)), device_id_type=MESH)
        return carry

    lax.fori_loop(0, half - 1, greet_half, 0)

    my_rows = pl.ds(pl.multiple_of(me_sp * rows, rows), rows)

    def arrival(t, h, d):
        return (key_recv.at[h], query_recv.at[h, d], value_recv.at[h])[t]

    def local_copy(t, h):
        src, dst = sources[t]
        cols = pl.ds(pl.multiple_of((me_sp * heads_here + h) * VD, VD), VD)
        return pltpu.make_async_copy(src.at[:, cols], dst.at[h, my_rows, :], arrival(t, h, 0))

    def outgoing(t, h, d):
        src, dst = sources[t]
        to = lax.rem(me_sp + d, count_sp)
        cols = pl.ds(pl.multiple_of((to * heads_here + h) * VD, VD), VD)
        return pltpu.make_async_remote_copy(
            src_ref=src.at[:, cols],
            dst_ref=dst.at[h, my_rows, :],
            send_sem=send_sem,
            recv_sem=arrival(t, h, d),
            device_id={"sp": to},
            device_id_type=MESH,
        )

    def landed(ref, sem):
        pltpu.make_async_copy(ref, ref, sem).wait()

    def table(t, n, slot):
        src, dst = ((routes_ref, routes_far), (weights_ref, weights_far))[t]
        return pltpu.make_async_remote_copy(
            src_ref=src,
            dst_ref=dst.at[slot],
            send_sem=table_send.at[t, n],
            recv_sem=table_recv.at[slot, t],
            device_id=on_line((near_z, last_z)[n]),
            device_id_type=MESH,
        )

    def weight_copy(i):
        h, member = i // count_sp, lax.rem(i, count_sp)
        given = pl.ds(pl.multiple_of((member * heads_here + h) * VD, VD), VD)
        return pltpu.make_async_copy(
            ow_hbm.at[given], ow.at[pl.ds(pl.multiple_of(i * VD, VD), VD)], ow_sem
        )

    loads = [
        pltpu.make_async_copy(src, dst, weight_sem.at[j])
        for j, (src, dst) in enumerate(((gate_hbm, gate), (up_hbm, up), (down_hbm, down)))
    ]

    pl.semaphore_wait(barrier, count_sp - 1 + half - 1)
    for h in range(heads_here):

        for t in (0, 2, 1):
            if h == 0:
                stages[t].wait()

            def start_all(i, carry, t=t, h=h):
                outgoing(t, h, 1 + lax.rem(i + count_sp // 2 - 1, count_sp - 1)).start()
                return carry

            lax.fori_loop(0, count_sp - 1, start_all, 0)
            local_copy(t, h).start()
    for n in range(2):
        for t in range(2):
            table(t, n, 1 - inside).start()

    def start_weight(i, carry):
        weight_copy(i).start()
        return carry

    lax.fori_loop(0, HEADS, start_weight, 0)
    for load in loads:
        load.start()

    def set_tables(slot, routes, weights):
        masks = slot_masks(routes, base, count, half, capacity)
        picks[slot] = jnp.where(masks[0] | masks[1], 1.0, 0.0).astype(jnp.bfloat16)
        combine = (
            jnp.where(masks[0], weights[0:1, :], 0.0) + jnp.where(masks[1], weights[1:2, :], 0.0)
        ).T
        high = combine.astype(jnp.bfloat16)
        shares[slot, 0] = high
        shares[slot, 1] = (combine - high.astype(jnp.float32)).astype(jnp.bfloat16)

    set_tables(0, routes_ref[...], weights_ref[...])

    def returning(h, p):
        dst_cols = pl.ds(pl.multiple_of((h * count_sp + me_sp) * VD, VD), VD)
        held = outs.at[h, pl.ds(pl.multiple_of(p * rows, rows), rows), :]

        @pl.when(p != me_sp)
        def _():
            pltpu.make_async_remote_copy(
                src_ref=held,
                dst_ref=att.at[:, dst_cols],
                send_sem=back_send,
                recv_sem=back_recv.at[h],
                device_id={"sp": p},
                device_id_type=MESH,
            ).start()

        @pl.when(p == me_sp)
        def _():
            pltpu.make_async_copy(held, att.at[:, dst_cols], back_recv.at[h]).start()

    factor = HD ** (-0.5) * math.log2(math.e)
    lanes = lax.broadcasted_iota(jnp.int32, (rows, VD), 1)
    def attend(h, p):
        head = me_sp * heads_here + h
        lam = lam_ref[head]
        gain = gain_ref[pl.ds(head, 1), :]
        at = pl.ds(pl.multiple_of(p * rows, rows), rows)
        q = qh[h, at, :]
        zero = jnp.zeros_like(q)
        both = jnp.concatenate(
            [jnp.where(lanes < HD, q, zero), jnp.where(lanes < HD, zero, q)], axis=0
        )
        scores = lax.dot_general(
            both, kh[h], (((1,), (1,)), ((), ())), preferred_element_type=jnp.float32
        )
        top = jnp.max(scores, axis=1, keepdims=True)
        e = jnp.exp2((scores - top) * factor)
        norm = jnp.sum(e, axis=1, keepdims=True)
        norm_1, norm_2 = norm[:rows], norm[rows:]
        share = lam * norm_1 / norm_2
        mixed = (e[:rows] - share * e[rows:]).astype(jnp.bfloat16)
        head_out = jnp.dot(mixed, vh[h], preferred_element_type=jnp.float32) / norm_1
        normed = head_out * lax.rsqrt(jnp.mean(head_out * head_out, axis=-1, keepdims=True) + eps)
        return (normed * gain * 0.8).astype(jnp.bfloat16)

    for h in range(heads_here):

        def step(i, carry, h=h):
            places = []
            for n in range(2):
                d = lax.rem(2 * i + n + count_sp // 2, count_sp)
                p = lax.rem(me_sp + count_sp - d, count_sp)
                at = pl.ds(pl.multiple_of(p * rows, rows), rows)
                landed(qh.at[h, at, :], query_recv.at[h, d])
                places.append((p, at))
            blocks = [attend(h, p) for p, _ in places]
            for (p, at), block in zip(places, blocks):
                outs[h, at, :] = block
            for p, _ in places:
                returning(h, p)
            return carry

        with jax.named_scope("kv"):
            landed(kh.at[h], key_recv.at[h])
            landed(vh.at[h], value_recv.at[h])
        with jax.named_scope("steps"):
            lax.fori_loop(0, count_sp // 2, step, 0)

    for slot in range(2):
        for t in range(2):
            table(t, 0, slot).wait_recv()
        set_tables(1 + slot, routes_far[slot], weights_far[slot])

    landed(ow, ow_sem)
    others = (count_sp - 1) * heads_here * VD
    tile = 512
    deep = count_sp * VD

    def projection(h, cols):
        heads = slice(h * deep, (h + 1) * deep)
        return jnp.dot(att[:, heads], ow[heads, cols], preferred_element_type=jnp.float32)

    for h in range(heads_here - 1):
        landed(att.at[:, pl.ds(h * deep, deep)], back_recv.at[h])
        for j in range(D // tile):
            cols = slice(j * tile, (j + 1) * tile)
            so_far = residual_ref[:, cols].astype(jnp.float32) if h == 0 else total[:, cols]
            total[:, cols] = so_far + projection(h, cols)
    last = heads_here - 1
    with jax.named_scope("back"):
        landed(att.at[:, pl.ds(last * deep, deep)], back_recv.at[last])

    square = jnp.zeros((rows, 1), jnp.float32)
    for j in range(D // tile):
        cols = slice(j * tile, (j + 1) * tile)
        so_far = residual_ref[:, cols].astype(jnp.float32) if last == 0 else total[:, cols]
        middle = (so_far + projection(last, cols)).astype(jnp.bfloat16)
        mid[:, cols] = middle
        wide = middle.astype(jnp.float32)
        square = square + jnp.sum(wide * wide, axis=1, keepdims=True)
    scale = lax.rsqrt(square / D + eps)
    xin[...] = (mid[...].astype(jnp.float32) * scale * fgain_ref[...]).astype(jnp.bfloat16)

    def rows_of(i):
        return pl.ds(pl.multiple_of(i * capacity, capacity), capacity)

    def part(c):
        return pl.ds(c * span, span)

    def remote(src, dst, sent, got, target):
        return pltpu.make_async_remote_copy(
            src_ref=src,
            dst_ref=dst,
            send_sem=sent,
            recv_sem=got,
            device_id=target,
            device_id_type=MESH,
        )

    def cross(c):
        slot = 1 - inside
        return remote(
            xin.at[:, part(c)],
            far.at[slot, :, part(c)],
            far_send,
            far_recv.at[slot, c],
            on_line(near_z),
        )

    def crossed(k, c):
        landed(far.at[k, :, part(c)], far_recv.at[k, c])

    def go(c, q, own):
        return remote(
            buffer.at[rows_of(q), part(c)],
            received.at[rows_of(me), part(c)],
            go_send,
            go_recv.at[own, c],
            coords(q),
        )

    def ret(c, q):
        return remote(
            results.at[rows_of(q), part(c)],
            returned.at[rows_of(me), part(c)],
            ret_send,
            ret_recv.at[c],
            coords(q),
        )

    def relay(k, c):
        held = far.at[k, :, part(c)]
        return remote(held, held, relay_send, far_recv.at[k, c], on_line(mate_z))

    def far_go(k, c, j):
        return remote(
            far_buffer.at[k, rows_of(j), part(c)],
            far_received.at[k, rows_of(me_j), part(c)],
            fgo_send,
            fgo_recv.at[k, c],
            coords(me_z * plane + j),
        )

    def far_ret(k, c, j):
        return remote(
            far_results.at[k, rows_of(j), part(c)],
            far_returned.at[k, rows_of(me), part(c)],
            fret_send,
            fret_recv.at[k, c],
            coords(gate_z * plane + j),
        )

    def sum_out(k, c):
        return remote(
            partial.at[k, :, part(c)],
            inbox.at[:, part(c)],
            sum_send,
            sum_recv.at[c],
            on_line(near_z if k == 0 else last_z),
        )

    def sum_here(c):
        landed(inbox.at[:, part(c)], sum_recv.at[c])

    def own_in(c):
        return pltpu.make_async_copy(
            buffer.at[rows_of(me), part(c)], received.at[rows_of(me), part(c)], go_recv.at[1, c]
        )

    def own_out(c):
        return pltpu.make_async_copy(
            results.at[rows_of(me), part(c)], returned.at[rows_of(me), part(c)], ret_recv.at[c]
        )

    def far_own_in(k, c):
        return pltpu.make_async_copy(
            far_buffer.at[k, rows_of(me_j), part(c)],
            far_received.at[k, rows_of(me_j), part(c)],
            fgo_recv.at[k, c],
        )

    def far_own_out(k, c):
        return pltpu.make_async_copy(
            far_results.at[k, rows_of(me_j), part(c)],
            far_returned.at[k, rows_of(me), part(c)],
            fret_recv.at[k, c],
        )

    def each(first, last, do):
        def loop(i, carry):
            do(i)
            return carry

        lax.fori_loop(first, last, loop, 0)

    def peers(do):
        each(0, half - 1, lambda i: do(peer(i)))

    def mates(do):
        each(1, plane, lambda i: do(lax.rem(me_j + i, plane)))

    def cut(c):
        return slice(c * span, (c + 1) * span)

    def spread(c):
        buffer[:, cut(c)] = jnp.dot(
            picks[0], xin[:, cut(c)], preferred_element_type=jnp.float32
        ).astype(jnp.bfloat16)
        mates(lambda j: go(c, me_z * plane + j, 1).start())
        own_in(c).start()

    def across(c):
        far_z = 1 - me_z
        each(0, plane, lambda i: go(c, far_z * plane + lax.rem(me_j + i, plane), 0).start())

    plane_rows = plane * capacity
    my_plane = pl.ds(pl.multiple_of(me_z * plane_rows, plane_rows), plane_rows)

    def far_spread(k, relaying):
        for c in range(PARTS):
            crossed(k, c)
            if relaying:
                relay(k, c).start()
            far_buffer[k, :, cut(c)] = jnp.dot(
                picks[1 + k, my_plane], far[k, :, cut(c)], preferred_element_type=jnp.float32
            ).astype(jnp.bfloat16)
            mates(lambda j, c=c: far_go(k, c, j).start())
            far_own_in(k, c).start()

    def expert(source, target, send):
        def make_hidden(j, carry):
            cols = pl.ds(pl.multiple_of(j * 256, 256), 256)
            gate_part = jnp.dot(source[...], gate[:, cols], preferred_element_type=jnp.float32)
            up_part = jnp.dot(source[...], up[:, cols], preferred_element_type=jnp.float32)
            hidden[:, cols] = (jax.nn.silu(gate_part) * up_part).astype(jnp.bfloat16)
            return carry

        lax.fori_loop(0, width // 256, make_hidden, 0)
        for c in range(PARTS):
            target[:, cut(c)] = jnp.dot(
                hidden[...], down[:, cut(c)], preferred_element_type=jnp.float32
            ).astype(jnp.bfloat16)
            send(c)

    def near_return(c, own):
        which = me_z if own else 1 - me_z
        if own:
            own_out(c).start()
            mates(lambda j: ret(c, which * plane + j).start())
        else:
            each(0, plane, lambda i: ret(c, which * plane + lax.rem(me_j + i, plane)).start())

    def near_batch(own, later=False):
        which = me_z if own else 1 - me_z
        at = pl.ds(pl.multiple_of(which * plane_rows, plane_rows), plane_rows)
        for c in range(PARTS):
            landed(received.at[at, part(c)], go_recv.at[1 if own else 0, c])

        def send(c):
            if not later:
                near_return(c, own)

        expert(received.at[at], results.at[at], send)

    def far_batch(k, inner_side):
        for c in range(PARTS):
            landed(far_received.at[k, :, part(c)], fgo_recv.at[k, c])

        def send(c):
            if inner_side:
                far_own_out(k, c).start()
            else:
                far_ret(k, c, me_j).start()
            mates(lambda j: far_ret(k, c, j).start())

        expert(far_received.at[k], far_results.at[k], send)

    def summed(slot, block):
        return jnp.dot(shares[slot, 0], block, preferred_element_type=jnp.float32) + jnp.dot(
            shares[slot, 1], block, preferred_element_type=jnp.float32
        )

    def far_sums(k):
        for c in range(PARTS):
            landed(far_returned.at[k, :, part(c)], fret_recv.at[k, c])
            partial[k, :, cut(c)] = summed(1 + k, far_returned[k, :, cut(c)]).astype(jnp.bfloat16)
            sum_out(k, c).start()

    def near_sums():
        for c in range(PARTS):
            landed(returned.at[:, part(c)], ret_recv.at[c])
            total[:, cut(c)] = mid[:, cut(c)].astype(jnp.float32) + summed(0, returned[:, cut(c)])

    for load in loads:
        load.wait()

    @pl.when(inside == 1)
    def _():
        with jax.named_scope("go"):
            for c in range(PARTS):
                spread(c)
                cross(c).start()
        with jax.named_scope("d1"):
            far_spread(0, True)
        with jax.named_scope("own"):
            near_batch(True)
        with jax.named_scope("d2"):
            far_spread(1, True)
        with jax.named_scope("ac"):
            for c in range(PARTS):
                across(c)
        with jax.named_scope("mate"):
            near_batch(False, True)
        with jax.named_scope("rt"):
            for c in range(PARTS):
                near_return(c, False)
        with jax.named_scope("b1"):
            far_batch(0, True)
        with jax.named_scope("b2"):
            far_batch(1, True)
        with jax.named_scope("s1"):
            far_sums(0)
        with jax.named_scope("s2"):
            far_sums(1)
        with jax.named_scope("near"):
            near_sums()

    @pl.when(inside == 0)
    def _():
        with jax.named_scope("go"):
            for c in range(PARTS):
                spread(c)
                across(c)
        with jax.named_scope("cr"):
            for c in range(PARTS):
                cross(c).start()
        with jax.named_scope("own"):
            near_batch(True)
        with jax.named_scope("d1"):
            far_spread(0, False)
        with jax.named_scope("b1"):
            far_batch(0, False)
        with jax.named_scope("d2"):
            far_spread(1, False)
        with jax.named_scope("b2"):
            far_batch(1, False)
        with jax.named_scope("mate"):
            near_batch(False)
        with jax.named_scope("near"):
            near_sums()

    with jax.named_scope("end"):
        for c in range(PARTS):
            sum_here(c)
            out_ref[:, cut(c)] = (total[:, cut(c)] + inbox[:, cut(c)].astype(jnp.float32)).astype(
                jnp.bfloat16
            )

    with jax.named_scope("drain"):
        for n in range(2):
            for t in range(2):
                table(t, n, 1 - inside).wait_send()

        def gone(ref, sem):
            remote(ref, ref, sem, sum_recv.at[0], on_line(near_z)).wait_send()

        gone(staged.at[:, :, pl.ds(0, others)], send_sem)
        gone(outs.at[:, pl.ds(0, (count_sp - 1) * rows), :], back_send)
        gone(buffer.at[pl.ds(0, (half - 1) * capacity)], go_send)
        gone(results.at[pl.ds(0, (half - 1) * capacity)], ret_send)
        gone(far_buffer.at[:, pl.ds(0, (plane - 1) * capacity)], fgo_send)
        gone(xin, far_send)

        @pl.when(inside == 0)
        def _():
            gone(far_results, fret_send)

        @pl.when(inside == 1)
        def _():
            gone(far_results.at[:, pl.ds(0, (plane - 1) * capacity)], fret_send)
            gone(far, relay_send)
            gone(partial, sum_send)


def kernels_on_device(
    residual,
    query_maps,
    key_maps,
    value_rows,
    lambdas,
    head_gain,
    out_weight,
    ffn_gain,
    routes,
    route_weights,
    expert_gate,
    expert_up,
    expert_down,
):
    count_sp = lax.axis_size("sp")
    count_dp = lax.axis_size("dp")
    experts_all = count_sp * count_dp
    rows = residual.shape[1]
    capacity = max(2, 4 * rows // experts_all)
    if capacity % 16 or count_sp % LINE:
        return on_device(
            residual,
            query_maps,
            key_maps,
            value_rows,
            lambdas,
            head_gain,
            out_weight,
            ffn_gain,
            routes,
            route_weights,
            expert_gate,
            expert_up,
            expert_down,
        )
    heads_here = HEADS // count_sp
    half = experts_all // 2
    plane = half // 2
    slots = half * capacity
    vmem = pl.BlockSpec(memory_space=pltpu.VMEM)
    hbm = pl.BlockSpec(memory_space=pl.ANY)
    dma = pltpu.SemaphoreType.DMA
    bf16, f32 = jnp.bfloat16, jnp.float32
    length = rows * count_sp
    width = expert_gate.shape[2]
    top = routes.shape[2]
    out = pl.pallas_call(
        functools.partial(layer_kernel, count_sp, count_dp, capacity),
        out_shape=jax.ShapeDtypeStruct((rows, D), bf16),
        in_specs=[pl.BlockSpec(memory_space=pltpu.SMEM), hbm, hbm, hbm, vmem, vmem, hbm, vmem]
        + [vmem, vmem, hbm, hbm, hbm],
        out_specs=vmem,
        scratch_shapes=[
            pltpu.VMEM((3, rows, D), bf16),
            pltpu.VMEM((heads_here, length, VD), bf16),
            pltpu.VMEM((heads_here, length, VD), bf16),
            pltpu.VMEM((heads_here, length, VD), bf16),
            pltpu.VMEM((heads_here, length, VD), bf16),
            pltpu.VMEM((rows, HEADS * VD), bf16),
            pltpu.VMEM(out_weight.shape, bf16),
            pltpu.VMEM((rows, D), bf16),
            pltpu.VMEM((rows, D), bf16),
            pltpu.VMEM((2, top, rows), jnp.int32),
            pltpu.VMEM((2, top, rows), f32),
            pltpu.VMEM((3, slots, rows), bf16),
            pltpu.VMEM((3, 2, rows, slots), bf16),
            pltpu.VMEM((2, rows, D), bf16),
            pltpu.VMEM((2, rows, D), bf16),
            pltpu.VMEM((rows, D), bf16),
            pltpu.VMEM((rows, D), f32),
            pltpu.VMEM((slots, D), bf16),
            pltpu.VMEM((slots, D), bf16),
            pltpu.VMEM((slots, D), bf16),
            pltpu.VMEM((slots, D), bf16),
            pltpu.VMEM((2, slots // 2, D), bf16),
            pltpu.VMEM((2, slots // 2, D), bf16),
            pltpu.VMEM((2, slots // 2, D), bf16),
            pltpu.VMEM((2, slots, D), bf16),
            pltpu.VMEM((D, width), bf16),
            pltpu.VMEM((D, width), bf16),
            pltpu.VMEM((width, D), bf16),
            pltpu.VMEM((slots // 2, width), bf16),
            dma,
            dma((heads_here,)),
            dma((heads_here, count_sp)),
            dma((heads_here,)),
            dma,
            dma((heads_here,)),
            dma,
            dma((3,)),
            dma((2, 2)),
            dma((2, 2)),
            dma,
            dma((2, PARTS)),
            dma,
            dma,
            dma((PARTS,)),
            dma,
            dma((2, PARTS)),
            dma,
            dma((PARTS,)),
            dma,
            dma((2, PARTS)),
            dma,
            dma((2, PARTS)),
            dma((3,)),
        ],
        compiler_params=pltpu.CompilerParams(
            collective_id=0, has_side_effects=True, vmem_limit_bytes=VMEM_LIMIT
        ),
    )(
        lambdas,
        query_maps[0],
        key_maps[0],
        value_rows[0],
        residual[0],
        head_gain.reshape(HEADS, VD),
        out_weight,
        ffn_gain.reshape(1, D),
        routes[0].T,
        route_weights[0].T,
        expert_gate[0],
        expert_up[0],
        expert_down[0],
    )
    return out[None]


def solution(mesh):
    return jax.shard_map(
        kernels_on_device,
        mesh=mesh,
        in_specs=(
            P("dp", "sp", None),
            P("dp", "sp", None),
            P("dp", "sp", None),
            P("dp", "sp", None),
            P(),
            P(),
            P(),
            P(),
            P("dp", "sp", None),
            P("dp", "sp", None),
            P(("sp", "dp"), None, None),
            P(("sp", "dp"), None, None),
            P(("sp", "dp"), None, None),
        ),
        out_specs=P("dp", "sp", None),
        check_vma=False,
    )
```

```python
import functools
import math

import jax
import jax.numpy as jnp
from jax import lax
from jax.experimental import pallas as pl
from jax.experimental.pallas import tpu as pltpu
from jax.sharding import PartitionSpec as P

D = 2048
HEADS = 16
HD = 64
VD = 128


eps = 1e-06


def attend_head(query_head, key_head, value_head, lam_head, gain_head):
    length = query_head.shape[0]
    block_rows = min(512, length)
    count_blocks = length // block_rows
    scaling = query_head.shape[-1] ** (-0.5)
    query_blocks = query_head.reshape(count_blocks, block_rows, 2, query_head.shape[-1])

    def one_block(query_block):
        scores = (
            jnp.einsum("qmd,kmd->mqk", query_block, key_head, preferred_element_type=jnp.float32)
            * scaling
        )
        probabilities = jax.nn.softmax(scores, axis=-1)
        mixed_map = (probabilities[0] - lam_head * probabilities[1]).astype(jnp.bfloat16)
        head_out = jnp.dot(mixed_map, value_head, preferred_element_type=jnp.float32)
        normed = head_out * lax.rsqrt(jnp.mean(head_out * head_out, axis=-1, keepdims=True) + eps)
        return (normed * gain_head * 0.8).astype(jnp.bfloat16)

    return lax.map(one_block, query_blocks).reshape(length, value_head.shape[-1])


def on_device(
    residual,
    query_maps,
    key_maps,
    value_rows,
    lambdas,
    head_gain,
    out_weight,
    ffn_gain,
    routes,
    route_weights,
    expert_gate,
    expert_up,
    expert_down,
):
    count_sp = lax.axis_size("sp")
    count_dp = lax.axis_size("dp")
    heads_here = HEADS // count_sp
    queries, keys_all, values_all = (
        lax.all_to_all(query_maps, "sp", split_axis=2, concat_axis=1, tiled=True),
        lax.all_to_all(key_maps, "sp", split_axis=2, concat_axis=1, tiled=True),
        lax.all_to_all(value_rows, "sp", split_axis=2, concat_axis=1, tiled=True),
    )
    first_head = lax.axis_index("sp") * heads_here
    lam_here = lax.dynamic_slice_in_dim(lambdas, first_head, heads_here)
    gain_here = lax.dynamic_slice_in_dim(head_gain, first_head * VD, heads_here * VD)
    outputs = []
    for head_index in range(heads_here):
        query_head = queries[0, :, head_index * 2 * HD : (head_index + 1) * 2 * HD].reshape(
            -1, 2, HD
        )
        key_head = keys_all[0, :, head_index * 2 * HD : (head_index + 1) * 2 * HD].reshape(
            -1, 2, HD
        )
        value_head = values_all[0, :, head_index * VD : (head_index + 1) * VD]
        gain_head = gain_here[head_index * VD : (head_index + 1) * VD]
        outputs.append(
            attend_head(query_head, key_head, value_head, lam_here[head_index], gain_head)
        )
    attended = jnp.concatenate(outputs, axis=1)[None]
    returned_heads = lax.all_to_all(attended, "sp", split_axis=1, concat_axis=2, tiled=True)
    projected = jnp.dot(returned_heads[0], out_weight, preferred_element_type=jnp.float32)
    residual_mid = (residual[0].astype(jnp.float32) + projected).astype(jnp.bfloat16)
    middle = residual_mid.astype(jnp.float32)
    expert_input = (
        middle * lax.rsqrt(jnp.mean(middle * middle, axis=-1, keepdims=True) + eps) * ffn_gain
    ).astype(jnp.bfloat16)
    tok_rows = residual.shape[1]
    experts_all = count_sp * count_dp
    capacity = max(2, 4 * tok_rows // experts_all)
    flat_routes = routes[0].reshape(-1)
    flat_weights = route_weights[0].reshape(-1)
    onehot = (flat_routes[:, None] == jnp.arange(experts_all, dtype=jnp.int32)[None, :]).astype(
        jnp.int32
    )
    before = jnp.cumsum(onehot, axis=0) - onehot
    rank_of = jnp.sum(before * onehot, axis=1)
    slot = flat_routes * capacity + rank_of
    token_of = jnp.arange(flat_routes.shape[0], dtype=jnp.int32) // routes.shape[2]
    slot_token = jnp.full((experts_all * capacity,), tok_rows, jnp.int32).at[slot].set(token_of)
    padded_input = jnp.concatenate([expert_input, jnp.zeros((1, D), jnp.bfloat16)], axis=0)
    buffer = padded_input[slot_token].reshape(experts_all, capacity, D)
    received = lax.all_to_all(buffer, ("sp", "dp"), split_axis=0, concat_axis=0, tiled=True)
    row_block = received.reshape(-1, D)
    gate_part = jnp.dot(row_block, expert_gate[0], preferred_element_type=jnp.float32)
    up_part = jnp.dot(row_block, expert_up[0], preferred_element_type=jnp.float32)
    hidden = (jax.nn.silu(gate_part) * up_part).astype(jnp.bfloat16)
    expert_out = jnp.dot(hidden, expert_down[0], preferred_element_type=jnp.float32).astype(
        jnp.bfloat16
    )
    returned = lax.all_to_all(
        expert_out.reshape(received.shape), ("sp", "dp"), split_axis=0, concat_axis=0, tiled=True
    )
    picked = returned.reshape(experts_all * capacity, D)[slot]
    weighted = (picked.astype(jnp.float32) * flat_weights[:, None]).reshape(
        tok_rows, routes.shape[2], D
    )
    layer_out = (middle + jnp.sum(weighted, axis=1)).astype(jnp.bfloat16)
    return layer_out[None]


MESH = pl.DeviceIdType.MESH
VMEM_LIMIT = 60 * 1024 * 1024


def slot_masks(routes, first_expert, experts_all, experts_here, capacity):
    rows = routes.shape[1]
    first, second = routes[0:1, :], routes[1:2, :]
    experts = lax.broadcasted_iota(jnp.int32, (experts_all, rows), 0)
    named_first, named_second = experts == first, experts == second
    named = jnp.where(named_first | named_second, 1.0, 0.0).astype(jnp.bfloat16)
    earlier = lax.broadcasted_iota(jnp.int32, (rows, rows), 0) < lax.broadcasted_iota(
        jnp.int32, (rows, rows), 1
    )
    before = jnp.dot(
        named, jnp.where(earlier, 1.0, 0.0).astype(jnp.bfloat16), preferred_element_type=jnp.float32
    )
    slots = lax.broadcasted_iota(jnp.int32, (experts_here * capacity, rows), 0)
    masks = []
    for route, chosen in ((first, named_first), (second, named_second)):
        rank = jnp.sum(jnp.where(chosen, before, 0.0), axis=0, keepdims=True).astype(jnp.int32)
        masks.append(slots == (route - first_expert) * capacity + rank)
    return masks


PARTS = 4
LINE = 4


def layer_kernel(
    count_sp,
    count_dp,
    capacity,
    lam_ref,
    q_ref,
    k_ref,
    v_ref,
    residual_ref,
    gain_ref,
    ow_hbm,
    fgain_ref,
    routes_ref,
    weights_ref,
    gate_hbm,
    up_hbm,
    down_hbm,
    out_ref,
    staged,
    qh,
    kh,
    vh,
    outs,
    att,
    ow,
    mid,
    xin,
    routes_far,
    weights_far,
    picks,
    shares,
    far,
    partial,
    inbox,
    total,
    buffer,
    received,
    results,
    returned,
    far_buffer,
    far_received,
    far_results,
    far_returned,
    gate,
    up,
    down,
    hidden,
    send_sem,
    key_recv,
    query_recv,
    value_recv,
    back_send,
    back_recv,
    ow_sem,
    weight_sem,
    table_send,
    table_recv,
    far_send,
    far_recv,
    relay_send,
    sum_send,
    sum_recv,
    go_send,
    go_recv,
    ret_send,
    ret_recv,
    fgo_send,
    fgo_recv,
    fret_send,
    fret_recv,
    stage_sem,
):
    me_sp = lax.axis_index("sp")
    rows = q_ref.shape[0]
    heads_here = HEADS // count_sp
    sources = ((staged.at[0], kh), (staged.at[1], qh), (staged.at[2], vh))
    stages = [
        pltpu.make_async_copy(src, staged.at[t], stage_sem.at[t])
        for t, src in enumerate((k_ref, q_ref, v_ref))
    ]
    for t in (0, 2, 1):
        stages[t].start()

    count = count_sp * count_dp
    inner = count_sp // LINE
    half = count // 2
    plane = half // 2
    z, y = me_sp // inner, lax.rem(me_sp, inner)
    side = z // 2
    base = side * half
    me = me_sp * count_dp + lax.axis_index("dp") - base
    me_z, me_j = me // plane, lax.rem(me, plane)
    inside = (z * (LINE - 1 - z)) // 2
    gate_z = 1 - side
    mate_z = z + 1 - 2 * lax.rem(z, 2)
    near_z = 2 - side
    last_z = 3 - 3 * side
    width = gate.shape[1]
    span = D // PARTS
    chunk = width // 2

    def coords(p):
        return {"sp": (base + p) // count_dp, "dp": lax.rem(base + p, count_dp)}

    def on_line(other):
        return {"sp": other * inner + y}

    def peer(i):
        e = i + i // plane
        return lax.rem(me_z + 1 + e // plane, 2) * plane + lax.rem(me_j + e, plane)

    barrier = pltpu.get_barrier_semaphore()

    def greet(d, carry):
        pl.semaphore_signal(
            barrier, inc=1, device_id={"sp": lax.rem(me_sp + d, count_sp)}, device_id_type=MESH
        )
        return carry

    lax.fori_loop(1, count_sp, greet, 0)

    def greet_half(i, carry):
        pl.semaphore_signal(barrier, inc=1, device_id=coords(peer(i)), device_id_type=MESH)
        return carry

    lax.fori_loop(0, half - 1, greet_half, 0)

    my_rows = pl.ds(pl.multiple_of(me_sp * rows, rows), rows)

    def arrival(t, h, d):
        return (key_recv.at[h], query_recv.at[h, d], value_recv.at[h])[t]

    def local_copy(t, h):
        src, dst = sources[t]
        cols = pl.ds(pl.multiple_of((me_sp * heads_here + h) * VD, VD), VD)
        return pltpu.make_async_copy(src.at[:, cols], dst.at[h, my_rows, :], arrival(t, h, 0))

    def outgoing(t, h, d):
        src, dst = sources[t]
        to = lax.rem(me_sp + d, count_sp)
        cols = pl.ds(pl.multiple_of((to * heads_here + h) * VD, VD), VD)
        return pltpu.make_async_remote_copy(
            src_ref=src.at[:, cols],
            dst_ref=dst.at[h, my_rows, :],
            send_sem=send_sem,
            recv_sem=arrival(t, h, d),
            device_id={"sp": to},
            device_id_type=MESH,
        )

    def landed(ref, sem):
        pltpu.make_async_copy(ref, ref, sem).wait()

    def table(t, n, slot):
        src, dst = ((routes_ref, routes_far), (weights_ref, weights_far))[t]
        return pltpu.make_async_remote_copy(
            src_ref=src,
            dst_ref=dst.at[slot],
            send_sem=table_send.at[t, n],
            recv_sem=table_recv.at[slot, t],
            device_id=on_line((near_z, last_z)[n]),
            device_id_type=MESH,
        )

    def weight_copy(i):
        h, member = i // count_sp, lax.rem(i, count_sp)
        given = pl.ds(pl.multiple_of((member * heads_here + h) * VD, VD), VD)
        return pltpu.make_async_copy(
            ow_hbm.at[given], ow.at[pl.ds(pl.multiple_of(i * VD, VD), VD)], ow_sem
        )

    loads = [
        pltpu.make_async_copy(src, dst, weight_sem.at[j])
        for j, (src, dst) in enumerate(((gate_hbm, gate), (up_hbm, up), (down_hbm, down)))
    ]

    pl.semaphore_wait(barrier, count_sp - 1 + half - 1)
    for h in range(heads_here):

        for t in (0, 2, 1):
            if h == 0:
                stages[t].wait()

            def start_all(i, carry, t=t, h=h):
                outgoing(t, h, 1 + lax.rem(i + count_sp // 2 - 1, count_sp - 1)).start()
                return carry

            lax.fori_loop(0, count_sp - 1, start_all, 0)
            local_copy(t, h).start()
    for n in range(2):
        for t in range(2):
            table(t, n, 1 - inside).start()

    def start_weight(i, carry):
        weight_copy(i).start()
        return carry

    lax.fori_loop(0, HEADS, start_weight, 0)
    for load in loads:
        load.start()

    def set_tables(slot, routes, weights):
        masks = slot_masks(routes, base, count, half, capacity)
        picks[slot] = jnp.where(masks[0] | masks[1], 1.0, 0.0).astype(jnp.bfloat16)
        combine = (
            jnp.where(masks[0], weights[0:1, :], 0.0) + jnp.where(masks[1], weights[1:2, :], 0.0)
        ).T
        high = combine.astype(jnp.bfloat16)
        shares[slot, 0] = high
        shares[slot, 1] = (combine - high.astype(jnp.float32)).astype(jnp.bfloat16)

    set_tables(0, routes_ref[...], weights_ref[...])

    def returning(h, p):
        dst_cols = pl.ds(pl.multiple_of((h * count_sp + me_sp) * VD, VD), VD)
        held = outs.at[h, pl.ds(pl.multiple_of(p * rows, rows), rows), :]

        @pl.when(p != me_sp)
        def _():
            pltpu.make_async_remote_copy(
                src_ref=held,
                dst_ref=att.at[:, dst_cols],
                send_sem=back_send,
                recv_sem=back_recv.at[h],
                device_id={"sp": p},
                device_id_type=MESH,
            ).start()

        @pl.when(p == me_sp)
        def _():
            pltpu.make_async_copy(held, att.at[:, dst_cols], back_recv.at[h]).start()

    factor = HD ** (-0.5) * math.log2(math.e)
    lanes = lax.broadcasted_iota(jnp.int32, (rows, VD), 1)
    def attend(h, p):
        head = me_sp * heads_here + h
        lam = lam_ref[head]
        gain = gain_ref[pl.ds(head, 1), :]
        at = pl.ds(pl.multiple_of(p * rows, rows), rows)
        q = qh[h, at, :]
        zero = jnp.zeros_like(q)
        both = jnp.concatenate(
            [jnp.where(lanes < HD, q, zero), jnp.where(lanes < HD, zero, q)], axis=0
        )
        scores = lax.dot_general(
            both, kh[h], (((1,), (1,)), ((), ())), preferred_element_type=jnp.float32
        )
        top = jnp.max(scores, axis=1, keepdims=True)
        e = jnp.exp2((scores - top) * factor)
        norm = jnp.sum(e, axis=1, keepdims=True)
        norm_1, norm_2 = norm[:rows], norm[rows:]
        share = lam * norm_1 / norm_2
        mixed = (e[:rows] - share * e[rows:]).astype(jnp.bfloat16)
        head_out = jnp.dot(mixed, vh[h], preferred_element_type=jnp.float32) / norm_1
        normed = head_out * lax.rsqrt(jnp.mean(head_out * head_out, axis=-1, keepdims=True) + eps)
        return (normed * gain * 0.8).astype(jnp.bfloat16)

    for h in range(heads_here):

        def step(i, carry, h=h):
            places = []
            for n in range(2):
                d = lax.rem(2 * i + n + count_sp // 2, count_sp)
                p = lax.rem(me_sp + count_sp - d, count_sp)
                at = pl.ds(pl.multiple_of(p * rows, rows), rows)
                landed(qh.at[h, at, :], query_recv.at[h, d])
                places.append((p, at))
            blocks = [attend(h, p) for p, _ in places]
            for (p, at), block in zip(places, blocks):
                outs[h, at, :] = block
            for p, _ in places:
                returning(h, p)
            return carry

        with jax.named_scope("kv"):
            landed(kh.at[h], key_recv.at[h])
            landed(vh.at[h], value_recv.at[h])
        with jax.named_scope("steps"):
            lax.fori_loop(0, count_sp // 2, step, 0)

    for slot in range(2):
        for t in range(2):
            table(t, 0, slot).wait_recv()
        set_tables(1 + slot, routes_far[slot], weights_far[slot])

    landed(ow, ow_sem)
    others = (count_sp - 1) * heads_here * VD
    tile = 512
    deep = count_sp * VD

    def projection(h, cols):
        heads = slice(h * deep, (h + 1) * deep)
        return jnp.dot(att[:, heads], ow[heads, cols], preferred_element_type=jnp.float32)

    for h in range(heads_here - 1):
        landed(att.at[:, pl.ds(h * deep, deep)], back_recv.at[h])
        for j in range(D // tile):
            cols = slice(j * tile, (j + 1) * tile)
            so_far = residual_ref[:, cols].astype(jnp.float32) if h == 0 else total[:, cols]
            total[:, cols] = so_far + projection(h, cols)
    last = heads_here - 1
    with jax.named_scope("back"):
        landed(att.at[:, pl.ds(last * deep, deep)], back_recv.at[last])

    square = jnp.zeros((rows, 1), jnp.float32)
    for j in range(D // tile):
        cols = slice(j * tile, (j + 1) * tile)
        so_far = residual_ref[:, cols].astype(jnp.float32) if last == 0 else total[:, cols]
        middle = (so_far + projection(last, cols)).astype(jnp.bfloat16)
        mid[:, cols] = middle
        wide = middle.astype(jnp.float32)
        square = square + jnp.sum(wide * wide, axis=1, keepdims=True)
    scale = lax.rsqrt(square / D + eps)
    xin[...] = (mid[...].astype(jnp.float32) * scale * fgain_ref[...]).astype(jnp.bfloat16)

    def rows_of(i):
        return pl.ds(pl.multiple_of(i * capacity, capacity), capacity)

    def part(c):
        return pl.ds(c * span, span)

    def remote(src, dst, sent, got, target):
        return pltpu.make_async_remote_copy(
            src_ref=src,
            dst_ref=dst,
            send_sem=sent,
            recv_sem=got,
            device_id=target,
            device_id_type=MESH,
        )

    def cross(c):
        slot = 1 - inside
        return remote(
            xin.at[:, part(c)],
            far.at[slot, :, part(c)],
            far_send,
            far_recv.at[slot, c],
            on_line(near_z),
        )

    def crossed(k, c):
        landed(far.at[k, :, part(c)], far_recv.at[k, c])

    def go(c, q, own):
        return remote(
            buffer.at[rows_of(q), part(c)],
            received.at[rows_of(me), part(c)],
            go_send,
            go_recv.at[own, c],
            coords(q),
        )

    def ret(c, q):
        return remote(
            results.at[rows_of(q), part(c)],
            returned.at[rows_of(me), part(c)],
            ret_send,
            ret_recv.at[c],
            coords(q),
        )

    def relay(k, c):
        held = far.at[k, :, part(c)]
        return remote(held, held, relay_send, far_recv.at[k, c], on_line(mate_z))

    def far_go(k, c, j):
        return remote(
            far_buffer.at[k, rows_of(j), part(c)],
            far_received.at[k, rows_of(me_j), part(c)],
            fgo_send,
            fgo_recv.at[k, c],
            coords(me_z * plane + j),
        )

    def far_ret(k, c, j):
        return remote(
            far_results.at[k, rows_of(j), part(c)],
            far_returned.at[k, rows_of(me), part(c)],
            fret_send,
            fret_recv.at[k, c],
            coords(gate_z * plane + j),
        )

    def sum_out(k, c):
        return remote(
            partial.at[k, :, part(c)],
            inbox.at[:, part(c)],
            sum_send,
            sum_recv.at[c],
            on_line(near_z if k == 0 else last_z),
        )

    def sum_here(c):
        landed(inbox.at[:, part(c)], sum_recv.at[c])

    def own_in(c):
        return pltpu.make_async_copy(
            buffer.at[rows_of(me), part(c)], received.at[rows_of(me), part(c)], go_recv.at[1, c]
        )

    def own_out(c):
        return pltpu.make_async_copy(
            results.at[rows_of(me), part(c)], returned.at[rows_of(me), part(c)], ret_recv.at[c]
        )

    def far_own_in(k, c):
        return pltpu.make_async_copy(
            far_buffer.at[k, rows_of(me_j), part(c)],
            far_received.at[k, rows_of(me_j), part(c)],
            fgo_recv.at[k, c],
        )

    def far_own_out(k, c):
        return pltpu.make_async_copy(
            far_results.at[k, rows_of(me_j), part(c)],
            far_returned.at[k, rows_of(me), part(c)],
            fret_recv.at[k, c],
        )

    def each(first, last, do):
        def loop(i, carry):
            do(i)
            return carry

        lax.fori_loop(first, last, loop, 0)

    def peers(do):
        each(0, half - 1, lambda i: do(peer(i)))

    def mates(do):
        each(1, plane, lambda i: do(lax.rem(me_j + i, plane)))

    def cut(c):
        return slice(c * span, (c + 1) * span)

    def spread(c):
        buffer[:, cut(c)] = jnp.dot(
            picks[0], xin[:, cut(c)], preferred_element_type=jnp.float32
        ).astype(jnp.bfloat16)
        mates(lambda j: go(c, me_z * plane + j, 1).start())
        own_in(c).start()

    def across(c):
        far_z = 1 - me_z
        each(0, plane, lambda i: go(c, far_z * plane + lax.rem(me_j + i, plane), 0).start())

    plane_rows = plane * capacity
    my_plane = pl.ds(pl.multiple_of(me_z * plane_rows, plane_rows), plane_rows)

    def far_spread(k, relaying):
        for c in range(PARTS):
            crossed(k, c)
            if relaying:
                relay(k, c).start()
            far_buffer[k, :, cut(c)] = jnp.dot(
                picks[1 + k, my_plane], far[k, :, cut(c)], preferred_element_type=jnp.float32
            ).astype(jnp.bfloat16)
            mates(lambda j, c=c: far_go(k, c, j).start())
            far_own_in(k, c).start()

    def expert(source, target, send):
        def make_hidden(j, carry):
            cols = pl.ds(pl.multiple_of(j * chunk, chunk), chunk)
            gate_part = jnp.dot(source[...], gate[:, cols], preferred_element_type=jnp.float32)
            up_part = jnp.dot(source[...], up[:, cols], preferred_element_type=jnp.float32)
            hidden[:, cols] = (jax.nn.silu(gate_part) * up_part).astype(jnp.bfloat16)
            return carry

        lax.fori_loop(0, width // chunk, make_hidden, 0)
        for c in range(PARTS):
            target[:, cut(c)] = jnp.dot(
                hidden[...], down[:, cut(c)], preferred_element_type=jnp.float32
            ).astype(jnp.bfloat16)
            send(c)

    def near_return(c, own):
        which = me_z if own else 1 - me_z
        if own:
            own_out(c).start()
            mates(lambda j: ret(c, which * plane + j).start())
        else:
            each(0, plane, lambda i: ret(c, which * plane + lax.rem(me_j + i, plane)).start())

    def near_batch(own, later=False):
        which = me_z if own else 1 - me_z
        at = pl.ds(pl.multiple_of(which * plane_rows, plane_rows), plane_rows)
        for c in range(PARTS):
            landed(received.at[at, part(c)], go_recv.at[1 if own else 0, c])

        def send(c):
            if not later:
                near_return(c, own)

        expert(received.at[at], results.at[at], send)

    def far_batch(k, inner_side):
        for c in range(PARTS):
            landed(far_received.at[k, :, part(c)], fgo_recv.at[k, c])

        def send(c):
            if inner_side:
                far_own_out(k, c).start()
            else:
                far_ret(k, c, me_j).start()
            mates(lambda j: far_ret(k, c, j).start())

        expert(far_received.at[k], far_results.at[k], send)

    def summed(slot, block):
        return jnp.dot(shares[slot, 0], block, preferred_element_type=jnp.float32) + jnp.dot(
            shares[slot, 1], block, preferred_element_type=jnp.float32
        )

    def far_sums(k):
        for c in range(PARTS):
            landed(far_returned.at[k, :, part(c)], fret_recv.at[k, c])
            partial[k, :, cut(c)] = summed(1 + k, far_returned[k, :, cut(c)]).astype(jnp.bfloat16)
            sum_out(k, c).start()

    def near_sums():
        for c in range(PARTS):
            landed(returned.at[:, part(c)], ret_recv.at[c])
            total[:, cut(c)] = mid[:, cut(c)].astype(jnp.float32) + summed(0, returned[:, cut(c)])

    for load in loads:
        load.wait()

    @pl.when(inside == 1)
    def _():
        with jax.named_scope("go"):
            for c in range(PARTS):
                spread(c)
                cross(c).start()
        with jax.named_scope("d1"):
            far_spread(0, True)
        with jax.named_scope("own"):
            near_batch(True)
        with jax.named_scope("d2"):
            far_spread(1, True)
        with jax.named_scope("ac"):
            for c in range(PARTS):
                across(c)
        with jax.named_scope("mate"):
            near_batch(False, True)
        with jax.named_scope("rt"):
            for c in range(PARTS):
                near_return(c, False)
        with jax.named_scope("b1"):
            far_batch(0, True)
        with jax.named_scope("b2"):
            far_batch(1, True)
        with jax.named_scope("s1"):
            far_sums(0)
        with jax.named_scope("s2"):
            far_sums(1)
        with jax.named_scope("near"):
            near_sums()

    @pl.when(inside == 0)
    def _():
        with jax.named_scope("go"):
            for c in range(PARTS):
                spread(c)
                across(c)
        with jax.named_scope("cr"):
            for c in range(PARTS):
                cross(c).start()
        with jax.named_scope("own"):
            near_batch(True)
        with jax.named_scope("d1"):
            far_spread(0, False)
        with jax.named_scope("b1"):
            far_batch(0, False)
        with jax.named_scope("d2"):
            far_spread(1, False)
        with jax.named_scope("b2"):
            far_batch(1, False)
        with jax.named_scope("mate"):
            near_batch(False)
        with jax.named_scope("near"):
            near_sums()

    with jax.named_scope("end"):
        for c in range(PARTS):
            sum_here(c)
            out_ref[:, cut(c)] = (total[:, cut(c)] + inbox[:, cut(c)].astype(jnp.float32)).astype(
                jnp.bfloat16
            )

    with jax.named_scope("drain"):
        for n in range(2):
            for t in range(2):
                table(t, n, 1 - inside).wait_send()

        def gone(ref, sem):
            remote(ref, ref, sem, sum_recv.at[0], on_line(near_z)).wait_send()

        gone(staged.at[:, :, pl.ds(0, others)], send_sem)
        gone(outs.at[:, pl.ds(0, (count_sp - 1) * rows), :], back_send)
        gone(buffer.at[pl.ds(0, (half - 1) * capacity)], go_send)
        gone(results.at[pl.ds(0, (half - 1) * capacity)], ret_send)
        gone(far_buffer.at[:, pl.ds(0, (plane - 1) * capacity)], fgo_send)
        gone(xin, far_send)

        @pl.when(inside == 0)
        def _():
            gone(far_results, fret_send)

        @pl.when(inside == 1)
        def _():
            gone(far_results.at[:, pl.ds(0, (plane - 1) * capacity)], fret_send)
            gone(far, relay_send)
            gone(partial, sum_send)


def kernels_on_device(
    residual,
    query_maps,
    key_maps,
    value_rows,
    lambdas,
    head_gain,
    out_weight,
    ffn_gain,
    routes,
    route_weights,
    expert_gate,
    expert_up,
    expert_down,
):
    count_sp = lax.axis_size("sp")
    count_dp = lax.axis_size("dp")
    experts_all = count_sp * count_dp
    rows = residual.shape[1]
    capacity = max(2, 4 * rows // experts_all)
    if capacity % 16 or count_sp % LINE:
        return on_device(
            residual,
            query_maps,
            key_maps,
            value_rows,
            lambdas,
            head_gain,
            out_weight,
            ffn_gain,
            routes,
            route_weights,
            expert_gate,
            expert_up,
            expert_down,
        )
    heads_here = HEADS // count_sp
    half = experts_all // 2
    plane = half // 2
    slots = half * capacity
    vmem = pl.BlockSpec(memory_space=pltpu.VMEM)
    hbm = pl.BlockSpec(memory_space=pl.ANY)
    dma = pltpu.SemaphoreType.DMA
    bf16, f32 = jnp.bfloat16, jnp.float32
    length = rows * count_sp
    width = expert_gate.shape[2]
    top = routes.shape[2]
    out = pl.pallas_call(
        functools.partial(layer_kernel, count_sp, count_dp, capacity),
        out_shape=jax.ShapeDtypeStruct((rows, D), bf16),
        in_specs=[pl.BlockSpec(memory_space=pltpu.SMEM), hbm, hbm, hbm, vmem, vmem, hbm, vmem]
        + [vmem, vmem, hbm, hbm, hbm],
        out_specs=vmem,
        scratch_shapes=[
            pltpu.VMEM((3, rows, D), bf16),
            pltpu.VMEM((heads_here, length, VD), bf16),
            pltpu.VMEM((heads_here, length, VD), bf16),
            pltpu.VMEM((heads_here, length, VD), bf16),
            pltpu.VMEM((heads_here, length, VD), bf16),
            pltpu.VMEM((rows, HEADS * VD), bf16),
            pltpu.VMEM(out_weight.shape, bf16),
            pltpu.VMEM((rows, D), bf16),
            pltpu.VMEM((rows, D), bf16),
            pltpu.VMEM((2, top, rows), jnp.int32),
            pltpu.VMEM((2, top, rows), f32),
            pltpu.VMEM((3, slots, rows), bf16),
            pltpu.VMEM((3, 2, rows, slots), bf16),
            pltpu.VMEM((2, rows, D), bf16),
            pltpu.VMEM((2, rows, D), bf16),
            pltpu.VMEM((rows, D), bf16),
            pltpu.VMEM((rows, D), f32),
            pltpu.VMEM((slots, D), bf16),
            pltpu.VMEM((slots, D), bf16),
            pltpu.VMEM((slots, D), bf16),
            pltpu.VMEM((slots, D), bf16),
            pltpu.VMEM((2, slots // 2, D), bf16),
            pltpu.VMEM((2, slots // 2, D), bf16),
            pltpu.VMEM((2, slots // 2, D), bf16),
            pltpu.VMEM((2, slots, D), bf16),
            pltpu.VMEM((D, width), bf16),
            pltpu.VMEM((D, width), bf16),
            pltpu.VMEM((width, D), bf16),
            pltpu.VMEM((slots // 2, width), bf16),
            dma,
            dma((heads_here,)),
            dma((heads_here, count_sp)),
            dma((heads_here,)),
            dma,
            dma((heads_here,)),
            dma,
            dma((3,)),
            dma((2, 2)),
            dma((2, 2)),
            dma,
            dma((2, PARTS)),
            dma,
            dma,
            dma((PARTS,)),
            dma,
            dma((2, PARTS)),
            dma,
            dma((PARTS,)),
            dma,
            dma((2, PARTS)),
            dma,
            dma((2, PARTS)),
            dma((3,)),
        ],
        compiler_params=pltpu.CompilerParams(
            collective_id=0, has_side_effects=True, vmem_limit_bytes=VMEM_LIMIT
        ),
    )(
        lambdas,
        query_maps[0],
        key_maps[0],
        value_rows[0],
        residual[0],
        head_gain.reshape(HEADS, VD),
        out_weight,
        ffn_gain.reshape(1, D),
        routes[0].T,
        route_weights[0].T,
        expert_gate[0],
        expert_up[0],
        expert_down[0],
    )
    return out[None]


def solution(mesh):
    return jax.shard_map(
        kernels_on_device,
        mesh=mesh,
        in_specs=(
            P("dp", "sp", None),
            P("dp", "sp", None),
            P("dp", "sp", None),
            P("dp", "sp", None),
            P(),
            P(),
            P(),
            P(),
            P("dp", "sp", None),
            P("dp", "sp", None),
            P(("sp", "dp"), None, None),
            P(("sp", "dp"), None, None),
            P(("sp", "dp"), None, None),
        ),
        out_specs=P("dp", "sp", None),
        check_vma=False,
    )
```
